256 devices in a mesh: sp: 32 (over z, y), tp: 8 (over x, core).
Axes of the slice: x: 4, y: 4, z: 8, core: 2. Of those that a mesh axis runs over, the one named last changes fastest.
Arguments:
- grouped_head_inputs: bfloat16 [32768, 2, 1024], P('sp', None, 'tp'), may hold values from -6 to 6
- head_gate_inputs: bfloat16 [32768, 2, 1024], P('sp', None, 'tp'), may hold values from -6 to 6
- unsmoothed_step: float32 [32768, 2, 16], P('sp', None, 'tp'), may hold values from -3.8 to 3.8
- head_decay_rate: float32 [2, 16], P(None, 'tp'), may hold values from 3.0517578e-06 to 0.04761905
- extra_log_decay: float32 [32768, 2, 16], P('sp', None, 'tp'), may hold values from -1.4 to 0
- first_group_keys: bfloat16 [32768, 128], P('sp'), may hold values from -6 to 6
- first_group_queries: bfloat16 [32768, 128], P('sp'), may hold values from -6 to 6
- second_group_keys: bfloat16 [32768, 64], P('sp'), may hold values from -6 to 6
- second_group_queries: bfloat16 [32768, 64], P('sp'), may hold values from -6 to 6
- head_input_filter: float32 [4, 2, 1024], P(None, None, 'tp'), may hold values from -3 to 3
- first_group_filter: float32 [4, 2, 128], replicated, may hold values from -3 to 3
- second_group_filter: float32 [4, 2, 64], replicated, may hold values from -3 to 3
- head_norm_gain: float32 [2, 1024], P(None, 'tp'), may hold values from 0.1 to 1.9
- output_weight: bfloat16 [2, 1024, 2048], P(None, None, 'tp'), may hold values from -0.125 to 0.125
- residual: bfloat16 [32768, 2048], P('sp', 'tp'), may hold values from -37 to 37
- channel_norm_gain: float32 [2048], replicated, may hold values from 0.1 to 1.9
- channel_gate_weight: bfloat16 [2048, 5120], P('sp', 'tp'), may hold values from -0.125 to 0.125
- channel_up_weight: bfloat16 [2048, 5120], P('sp', 'tp'), may hold values from -0.125 to 0.125
- channel_down_weight: bfloat16 [2048, 5120], P('sp', 'tp'), may hold values from -0.078125 to 0.078125
Outputs:
- layer_output: bfloat16 [32768, 2048], P('sp', 'tp')
The draws below stay inside these ranges and needn't reach their ends.
All inputs are finite; a program needn't handle non-finite values.
Results may differ from the reference program's by a relative error of at most 0.007.
Values may be sent and summed in bfloat16 or wider, within the bound.
No kernel may reach another device: no remote copies, remote signals or barrier semaphores. Data moves between devices by JAX's collectives and lax.ppermute only.
A program may use at most 128 MiB of HBM per device.

```python
import math
import jax
import jax.numpy as jnp
from jax import lax

D = 2048
GROUP_HEADS = 16
HEAD = 64
STATE_ONE = 128
STATE_TWO = 64
FF = 5120
CONV = 4
BLOCK = 128
TOKENS = 32768
CHANNELS = 1024
N_TP = 8


def draw_unsmoothed_step(key, part):
    noise_key = jax.random.fold_in(key, 11)
    block_key = jax.random.fold_in(key, 12)
    block_total = TOKENS // BLOCK
    offsets = jax.random.uniform(block_key, (block_total, 1, 1, 1), jnp.float32, -1.0, 1.0)
    noise = 0.7 * jax.random.truncated_normal(noise_key, -4.0, 4.0, (block_total, BLOCK, 2, GROUP_HEADS), jnp.float32)
    return (noise + offsets).reshape(TOKENS, 2, GROUP_HEADS)


def draw_head_decay_rate(key, part):
    choose_key = jax.random.fold_in(key, 21)
    fast_key = jax.random.fold_in(key, 22)
    slow_key = jax.random.fold_in(key, 23)
    share = 0.5
    quick = jax.random.uniform(choose_key, (2, GROUP_HEADS), jnp.float32) < share
    fast = jnp.exp(jax.random.uniform(fast_key, (2, GROUP_HEADS), jnp.float32, math.log(1.0 / 70.0), math.log(1.0 / 21.0)))
    slow = jnp.exp(jax.random.uniform(slow_key, (2, GROUP_HEADS), jnp.float32, math.log(0.1), math.log(0.6))) / TOKENS
    return jnp.where(quick, fast, slow)


def draw_extra_log_decay(key, part):
    place_key = jax.random.fold_in(key, 31)
    loss_key = jax.random.fold_in(key, 32)
    places = jax.random.randint(place_key, (2, 2, GROUP_HEADS), 0, TOKENS)
    losses = jax.random.uniform(loss_key, (2, 2, GROUP_HEADS), jnp.float32, 0.2, 0.5)
    positions = jnp.arange(TOKENS, dtype=jnp.int32)[:, None, None, None]
    struck = positions == places[None]
    return jnp.sum(jnp.where(struck, jnp.log(1.0 - losses)[None], 0.0), axis=1)


def draw_residual(key, part):
    row_key = jax.random.fold_in(key, 41)
    column_key = jax.random.fold_in(key, 42)
    noise_key = jax.random.fold_in(key, 43)
    row_scale = jnp.exp(jax.random.uniform(row_key, (TOKENS, 1), jnp.float32, math.log(0.3), math.log(3.0)))
    column_scale = jnp.exp(jax.random.uniform(column_key, (1, D), jnp.float32, math.log(0.3), math.log(3.0)))
    noise = jax.random.truncated_normal(noise_key, -4.0, 4.0, (TOKENS, D), jnp.float32)
    return (noise * row_scale * column_scale).astype(jnp.bfloat16)


def level_of(own_key, dims, cuts, least, high):
    def one(axis_at, parts):
        heights = jax.random.uniform(jax.random.fold_in(jax.random.fold_in(own_key, 6), axis_at), (parts,), jnp.float32, least / len(cuts), high / len(cuts))
        return jnp.repeat(jnp.exp(heights), dims[axis_at] // parts).reshape((-1,) + (1,) * (len(dims) - axis_at - 1))

    gain = one(*cuts[0])
    for cut in cuts[1:]:
        gain = gain * one(*cut)
    return gain


def normal_values(own_key, dims, width, bound, cuts=(), kind=jnp.bfloat16):
    level = level_of(own_key, dims, cuts, -0.22, 0.18) if cuts else 1.0
    entries = jax.random.normal(own_key, dims, jnp.float32) * width * level
    return jnp.minimum(jnp.maximum(entries, -bound), bound).astype(kind)


def setup_inputs(seed: int = 0) -> dict:
    key_list = jax.random.split(jax.random.key(seed), 20)
    grouped_head_inputs = normal_values(key_list[0], (TOKENS, 2, CHANNELS), 1.0, 6.0, ((0, 32), (2, 8)))
    head_gate_inputs = normal_values(key_list[1], (TOKENS, 2, CHANNELS), 1.0, 6.0, ((0, 32), (2, 8)))
    unsmoothed_step = draw_unsmoothed_step(jax.random.fold_in(key_list[19], 71), 0)
    head_decay_rate = draw_head_decay_rate(jax.random.fold_in(key_list[19], 71), 0)
    extra_log_decay = draw_extra_log_decay(jax.random.fold_in(key_list[19], 71), 0)
    first_group_keys = normal_values(key_list[5], (TOKENS, STATE_ONE), 1.0, 6.0, ((0, 32),))
    first_group_queries = normal_values(key_list[6], (TOKENS, STATE_ONE), 1.0, 6.0, ((0, 32),))
    second_group_keys = normal_values(key_list[7], (TOKENS, STATE_TWO), 1.0, 6.0, ((0, 32),))
    second_group_queries = normal_values(key_list[8], (TOKENS, STATE_TWO), 1.0, 6.0, ((0, 32),))
    head_input_filter = normal_values(key_list[9], (CONV, 2, CHANNELS), 0.5, 3.0, ((2, 8),), jnp.float32)
    first_group_filter = normal_values(key_list[10], (CONV, 2, STATE_ONE), 0.5, 3.0, (), jnp.float32)
    second_group_filter = normal_values(key_list[11], (CONV, 2, STATE_TWO), 0.5, 3.0, (), jnp.float32)
    head_norm_gain = jnp.clip(1.0 + 0.18 * jax.random.normal(key_list[12], (2, CHANNELS), jnp.float32), 0.1, 1.9)
    output_weight = normal_values(key_list[13], (2, CHANNELS, D), (2 * CHANNELS) ** -0.5, 0.125, ((2, 8),))
    residual = draw_residual(jax.random.fold_in(key_list[19], 71), 0)
    channel_norm_gain = jnp.clip(1.0 + 0.18 * jax.random.normal(key_list[15], (D,), jnp.float32), 0.1, 1.9)
    channel_gate_weight = normal_values(key_list[16], (D, FF), D ** -0.5, 0.125, ((0, 32), (1, 8)))
    channel_up_weight = normal_values(key_list[17], (D, FF), D ** -0.5, 0.125, ((0, 32), (1, 8)))
    channel_down_weight = normal_values(key_list[18], (D, FF), FF ** -0.5, 0.078125, ((0, 32), (1, 8)))
    return dict(grouped_head_inputs=grouped_head_inputs, head_gate_inputs=head_gate_inputs, unsmoothed_step=unsmoothed_step, head_decay_rate=head_decay_rate, extra_log_decay=extra_log_decay, first_group_keys=first_group_keys, first_group_queries=first_group_queries, second_group_keys=second_group_keys, second_group_queries=second_group_queries, head_input_filter=head_input_filter, first_group_filter=first_group_filter, second_group_filter=second_group_filter, head_norm_gain=head_norm_gain, output_weight=output_weight, residual=residual, channel_norm_gain=channel_norm_gain, channel_gate_weight=channel_gate_weight, channel_up_weight=channel_up_weight, channel_down_weight=channel_down_weight)


EPSILON = 1e-06
PRECISE = lax.Precision.HIGHEST

def causal_taps(values, taps):
    length = values.shape[0]
    zeros_rows = jnp.zeros((CONV - 1,) + values.shape[1:], jnp.float32)
    padded = jnp.concatenate([zeros_rows, values.astype(jnp.float32)], axis=0)
    running = jnp.zeros(values.shape, jnp.float32)
    for offset in range(CONV):
        running = running + taps[offset].astype(jnp.float32) * padded[offset:offset + length]
    return jax.nn.silu(running)

def block_pass(current, value_rows, log_rows, key_rows, query_rows):
    cumulative = jnp.cumsum(log_rows, axis=0)
    length = value_rows.shape[0]
    causal = jnp.arange(length)[:, None] >= jnp.arange(length)[None, :]
    scores = jnp.dot(query_rows, key_rows.T, precision=PRECISE)
    span_logs = jnp.where(causal[:, :, None], cumulative[:, None, :] - cumulative[None, :, :], -jnp.inf)
    weights = jnp.exp(span_logs) * scores[:, :, None]
    inside = jnp.einsum('lsh,shp->lhp', weights, value_rows, precision=PRECISE)
    carried = jnp.einsum('ls,hps->lhp', query_rows, current, precision=PRECISE) * jnp.exp(cumulative)[:, :, None]
    to_end = jnp.exp(cumulative[-1][None, :] - cumulative)
    update = jnp.einsum('lhp,ls->hps', value_rows * to_end[:, :, None], key_rows, precision=PRECISE)
    new_state = current * jnp.exp(cumulative[-1])[:, None, None] + update
    return (new_state, inside + carried)

def scan_group(value_rows, log_rows, key_rows, query_rows):
    length, head_count, head_width = value_rows.shape
    block_count = length // BLOCK
    initial = jnp.zeros((head_count, head_width, key_rows.shape[1]), jnp.float32)
    blocks = (value_rows.reshape(block_count, BLOCK, head_count, head_width), log_rows.reshape(block_count, BLOCK, head_count), key_rows.reshape(block_count, BLOCK, -1), query_rows.reshape(block_count, BLOCK, -1))

    def advance(current, pieces):
        return block_pass(current, pieces[0], pieces[1], pieces[2], pieces[3])
    final_state, outputs = lax.scan(advance, initial, blocks)
    return outputs.reshape(length, head_count, head_width)

def reference(grouped_head_inputs, head_gate_inputs, unsmoothed_step, head_decay_rate, extra_log_decay, first_group_keys, first_group_queries, second_group_keys, second_group_queries, head_input_filter, first_group_filter, second_group_filter, head_norm_gain, output_weight, residual, channel_norm_gain, channel_gate_weight, channel_up_weight, channel_down_weight):
    length = grouped_head_inputs.shape[0]
    conv_heads = causal_taps(grouped_head_inputs, head_input_filter)
    keys_one = causal_taps(first_group_keys, first_group_filter[:, 0])
    queries_one = causal_taps(first_group_queries, first_group_filter[:, 1])
    keys_two = causal_taps(second_group_keys, second_group_filter[:, 0])
    queries_two = causal_taps(second_group_queries, second_group_filter[:, 1])
    head_step_size = jax.nn.softplus(unsmoothed_step.astype(jnp.float32))
    decay_logarithm = extra_log_decay.astype(jnp.float32) - head_step_size * head_decay_rate.astype(jnp.float32)[None]
    values = conv_heads.reshape(length, 2, GROUP_HEADS, HEAD) * head_step_size[:, :, :, None]
    first = scan_group(values[:, 0], decay_logarithm[:, 0], keys_one, queries_one)
    second = scan_group(values[:, 1], decay_logarithm[:, 1], keys_two, queries_two)
    mixer = jnp.stack([first, second], axis=1)
    gated = mixer * jax.nn.silu(head_gate_inputs.astype(jnp.float32)).reshape(length, 2, GROUP_HEADS, HEAD)
    scaled = gated * lax.rsqrt(lax.optimization_barrier(jnp.mean(gated * gated, axis=3, keepdims=True)) + EPSILON)
    mixed = (scaled.reshape(length, 2, CHANNELS) * head_norm_gain.astype(jnp.float32)[None]).astype(jnp.bfloat16)
    projected = jnp.dot(mixed.reshape(length, 2 * CHANNELS), output_weight.reshape(2 * CHANNELS, D), preferred_element_type=jnp.float32)
    stream = (residual.astype(jnp.float32) + projected).astype(jnp.bfloat16)
    stream_wide = stream.astype(jnp.float32)
    normed = (stream_wide * lax.rsqrt(lax.optimization_barrier(jnp.mean(stream_wide * stream_wide, axis=1, keepdims=True)) + EPSILON) * channel_norm_gain.astype(jnp.float32)[None]).astype(jnp.bfloat16)
    gate = jnp.dot(normed, channel_gate_weight, preferred_element_type=jnp.float32)
    upward = jnp.dot(normed, channel_up_weight, preferred_element_type=jnp.float32)
    hidden = (jax.nn.silu(gate) * upward).astype(jnp.bfloat16)
    block_width = FF // N_TP
    summed = jnp.zeros((length, D), jnp.float32)
    for index in range(N_TP):
        piece = hidden[:, index * block_width:(index + 1) * block_width]
        columns = channel_down_weight[:, index * block_width:(index + 1) * block_width]
        partial_value = lax.dot_general(piece, columns, (((1,), (1,)), ((), ())), preferred_element_type=jnp.float32)
        rounded = lax.optimization_barrier(partial_value.astype(jnp.bfloat16))
        summed = summed + rounded.astype(jnp.float32)
    return (stream_wide + 0.5 * summed).astype(jnp.bfloat16)
```

```python
import jax
import jax.numpy as jnp
from jax import lax
from jax.experimental import pallas as pl
from jax.experimental.pallas import tpu as pltpu
from jax.sharding import Mesh, PartitionSpec as P


EPSILON = 1e-06
BLOCK = 128
F32 = jnp.float32
BF16 = jnp.bfloat16
SP = ("z", "y")
TP = ("x", "c")


def silu(v):
    return v * jax.nn.sigmoid(v)


def shape(dims, kind):
    return jax.ShapeDtypeStruct(dims, kind)


def pack_rim_body(x_ref, k1_ref, q1_ref, k2_ref, q2_ref, out_ref):
    out_ref[:, 0:256] = x_ref[...]
    out_ref[:, 256:384] = k1_ref[...]
    out_ref[:, 384:512] = q1_ref[...]
    both = jnp.concatenate([k2_ref[...], q2_ref[...]], axis=0).astype(F32)
    out_ref[:, 512:640] = both.T[112:128].astype(BF16)


def pack_rim(x_tail, k1, q1, k2t, q2t):
    rows = k1.shape[0] // 16 - 1
    cols = k2t.shape[1] // 128 - 1
    return pl.pallas_call(
        pack_rim_body,
        grid=(1,),
        in_specs=[
            pl.BlockSpec((16, 256), lambda i: (0, 0)),
            pl.BlockSpec((16, 128), lambda i: (rows, 0)),
            pl.BlockSpec((16, 128), lambda i: (rows, 0)),
            pl.BlockSpec((64, 128), lambda i: (0, cols)),
            pl.BlockSpec((64, 128), lambda i: (0, cols)),
        ],
        out_specs=pl.BlockSpec((16, 640), lambda i: (0, 0)),
        out_shape=shape((16, 640), BF16),
        name="pack_rim",
    )(x_tail, k1, q1, k2t, q2t)


def lanes_of(rows):
    return lax.broadcasted_iota(jnp.int32, (rows, 128), 1) < 64


def three_parts(v):
    hi = v.astype(BF16)
    rest = v - hi.astype(F32)
    mid = rest.astype(BF16)
    low = (rest - mid.astype(F32)).astype(BF16)
    return hi.astype(F32), mid.astype(F32), low.astype(F32)


def states_body(
    rate_ref, x_ref, k1_ref, q1_ref, k2_ref, q2_ref, rim_ref, filt_ref, step_ref, extra_ref,
    xc_ref, k1c_ref, q1c_ref, kq2c_ref, cum_ref, sp_ref, s1_ref, s2_ref, lead_ref, end_ref,
    buf,
):
    length = x_ref.shape[0]
    blocks = length // BLOCK
    upper = (
        lax.broadcasted_iota(jnp.int32, (BLOCK, BLOCK), 0)
        <= lax.broadcasted_iota(jnp.int32, (BLOCK, BLOCK), 1)
    ).astype(F32)
    steps, cums = [], []
    for head in range(4):
        raw = step_ref[head * 8 : head * 8 + 8, :]
        soft = jnp.maximum(raw, 0.0) + jnp.log1p(jnp.exp(-jnp.abs(raw)))
        logs = extra_ref[head * 8 : head * 8 + 8, :] - soft * rate_ref[head // 2, head % 2]
        total = jnp.dot(
            logs, upper, precision=lax.Precision.HIGHEST, preferred_element_type=F32
        )
        steps.append(soft)
        cums.append(total)
        cum_ref[head * 8 : head * 8 + 8, :] = total
        sp_ref[head * 8 : head * 8 + 8, :] = soft
    buf[0:8, :] = rim_ref[8:16, :].astype(F32)
    buf[8 : 8 + length, 0:256] = x_ref[...].astype(F32)
    buf[8 : 8 + length, 256:384] = k1_ref[...].astype(F32)
    buf[8 : 8 + length, 384:512] = q1_ref[...].astype(F32)
    for b in range(blocks):
        at = slice(b * BLOCK, (b + 1) * BLOCK)
        both = jnp.concatenate([k2_ref[:, at], q2_ref[:, at]], axis=0).astype(F32)
        buf[8 + b * BLOCK : 8 + (b + 1) * BLOCK, 512:640] = both.T
    first = lanes_of(1)
    state_one = jnp.zeros((128, 128), F32)
    state_two = jnp.zeros((64, 128), F32)
    lead_one = jnp.zeros((1, 128), F32)
    lead_two = jnp.zeros((1, 128), F32)
    s2_ref[...] = jnp.zeros(s2_ref.shape, BF16)
    for b in range(blocks):
        at = slice(b * BLOCK, (b + 1) * BLOCK)

        def conv(lo, hi):
            run = filt_ref[0:1, lo:hi] * buf[5 + b * BLOCK : 5 + (b + 1) * BLOCK, lo:hi]
            for k in range(1, 4):
                run = run + filt_ref[k : k + 1, lo:hi] * buf[
                    5 + k + b * BLOCK : 5 + k + (b + 1) * BLOCK, lo:hi
                ]
            return silu(run)

        x_one = conv(0, 128).astype(BF16)
        x_two = conv(128, 256).astype(BF16)
        xc_ref[at, 0:128] = x_one
        xc_ref[at, 128:256] = x_two
        k_one = conv(256, 384)
        k1c_ref[at, :] = k_one.astype(BF16)
        q1c_ref[at, :] = conv(384, 512).astype(BF16)
        kq_two = conv(512, 640)
        kq2c_ref[at, :] = kq_two.astype(BF16)
        s1_ref[at, :] = state_one.astype(BF16)
        s2_ref[b * BLOCK + 64 : (b + 1) * BLOCK, :] = state_two.astype(BF16)
        lead_ref[b : b + 1, :] = lead_one
        lead_ref[8 + b : 9 + b, :] = lead_two
        key_one = k_one.T
        key_two = kq_two.T[0:64]
        ups, tots = [], []
        for head in range(4):
            row = cums[head][b : b + 1, :]
            tot = row[:, 127:128]
            weight = jnp.exp(tot - row) * steps[head][b : b + 1, :]
            key = key_one if head < 2 else key_two
            ups.append(
                jnp.dot(
                    (key * weight).astype(BF16),
                    x_one if head < 2 else x_two,
                    preferred_element_type=F32,
                )
            )
            tots.append(jnp.broadcast_to(tot, (1, 128)))
        tot_one = jnp.where(first, tots[0], tots[1])
        tot_two = jnp.where(first, tots[2], tots[3])
        state_one = state_one * jnp.exp(tot_one) + jnp.where(first, ups[0], ups[1])
        state_two = state_two * jnp.exp(tot_two) + jnp.where(first, ups[2], ups[3])
        lead_one = lead_one + tot_one
        lead_two = lead_two + tot_two
    end_ref[0:128, :] = state_one.astype(BF16)
    end_ref[128:192, :] = state_two.astype(BF16)
    end_ref[192:208, :] = log_rows(lead_one, lead_two)


def log_rows(one, two):
    parts = three_parts(one) + three_parts(two)
    return jnp.concatenate(list(parts) + [jnp.zeros((10, 128), F32)], axis=0).astype(BF16)


def logs_in(payload_ref):
    rows = payload_ref[192:208, :].astype(F32)
    one = rows[0:1] + rows[1:2] + rows[2:3]
    two = rows[3:4] + rows[4:5] + rows[5:6]
    return one, two


def inside_body(xc_ref, k1_ref, q1_ref, kq2_ref, cum_ref, sp_ref, out_ref):
    length = xc_ref.shape[0]
    causal = lax.broadcasted_iota(jnp.int32, (BLOCK, BLOCK), 0) >= lax.broadcasted_iota(
        jnp.int32, (BLOCK, BLOCK), 1
    )
    columns = cum_ref[...].T
    first = lanes_of(1)
    contract = (((1,), (1,)), ((), ()))
    for b in range(length // BLOCK):
        at = slice(b * BLOCK, (b + 1) * BLOCK)
        kq_two = kq2_ref[at, :].astype(F32)
        query_two = jnp.where(first, 0.0, kq_two).astype(BF16)
        key_two = pltpu.roll(kq_two, 64, 1).astype(BF16)
        scores = (
            lax.dot_general(q1_ref[at, :], k1_ref[at, :], contract, preferred_element_type=F32),
            lax.dot_general(query_two, key_two, contract, preferred_element_type=F32),
        )
        for group in range(2):
            values = xc_ref[at, group * 128 : group * 128 + 128]
            parts = []
            for inner in range(2):
                row = (group * 2 + inner) * 8 + b
                spans = jnp.where(
                    causal, columns[:, row : row + 1] - cum_ref[row : row + 1, :], -jnp.inf
                )
                weights = jnp.exp(spans) * (scores[group] * sp_ref[row : row + 1, :])
                parts.append(jnp.dot(weights.astype(BF16), values, preferred_element_type=F32))
            out_ref[at, group * 128 : group * 128 + 128] = jnp.where(first, parts[0], parts[1])


def combine_body(y_ref, own_ref, b1_ref, b2_ref, b3_ref, pre_ref, lead_ref, total_ref):
    y = y_ref[0]
    refs = (own_ref, b1_ref, b2_ref, b3_ref)
    place = [lax.rem(y - k + 4, 4) for k in range(4)]
    logs = [logs_in(r) for r in refs]
    zero = jnp.zeros((1, 128), F32)

    def pick(flag, v):
        return jnp.where(flag, v, zero)

    leads = [zero, zero]
    pre_one = jnp.zeros((128, 128), F32)
    pre_two = jnp.zeros((64, 128), F32)
    tot_one = jnp.zeros((128, 128), F32)
    tot_two = jnp.zeros((64, 128), F32)
    for k in range(4):
        one = refs[k][0:128, :].astype(F32)
        two = refs[k][128:192, :].astype(F32)
        if k:
            flag = k <= y
            pre_one = pre_one + pick(flag, jnp.exp(leads[0])) * one
            pre_two = pre_two + pick(flag, jnp.exp(leads[1])) * two
            leads = [leads[g] + pick(flag, logs[k][g]) for g in range(2)]
        later = [zero, zero]
        for j in range(4):
            if j != k:
                flag = place[j] > place[k]
                later = [later[g] + pick(flag, logs[j][g]) for g in range(2)]
        tot_one = tot_one + jnp.exp(later[0]) * one
        tot_two = tot_two + jnp.exp(later[1]) * two
    pre_ref[0:128, :] = pre_one
    pre_ref[128:192, :] = pre_two
    lead_ref[0:1, :] = leads[0]
    lead_ref[1:2, :] = leads[1]
    total_ref[0:128, :] = tot_one.astype(BF16)
    total_ref[128:192, :] = tot_two.astype(BF16)
    total_ref[192:208, :] = log_rows(
        logs[0][0] + logs[1][0] + logs[2][0] + logs[3][0],
        logs[0][1] + logs[1][1] + logs[2][1] + logs[3][1],
    )


def mixed_body(
    c_ref, in_ref, gate_ref, q1_ref, kq2_ref, cum_ref, s1_ref, s2_ref, lead_ref, gain_ref,
    pre_ref, ylead_ref, *rest,
):
    rows_refs, (mine_ref, theirs_ref) = rest[:-2], rest[-2:]
    c = c_ref[0]
    far_one = jnp.zeros((128, 128), F32)
    far_two = jnp.zeros((64, 128), F32)
    run = [jnp.zeros((1, 128), F32)] * 2
    for r in rows_refs:
        far_one = far_one + jnp.exp(run[0]) * r[0:128, :].astype(F32)
        far_two = far_two + jnp.exp(run[1]) * r[128:192, :].astype(F32)
        logs = logs_in(r)
        run = [run[0] + logs[0], run[1] + logs[1]]
    enter = (
        pre_ref[0:128, :] + jnp.exp(ylead_ref[0:1, :]) * far_one,
        jnp.concatenate(
            [
                jnp.zeros((64, 128), F32),
                pre_ref[128:192, :] + jnp.exp(ylead_ref[1:2, :]) * far_two,
            ],
            axis=0,
        ),
    )
    columns = jnp.exp(cum_ref[...].T)
    first = lanes_of(1)
    same_head = (
        (lax.broadcasted_iota(jnp.int32, (128, 128), 0) < 64)
        == (lax.broadcasted_iota(jnp.int32, (128, 128), 1) < 64)
    ).astype(BF16)
    blocks = in_ref.shape[0] // BLOCK
    half = blocks // 2
    for b in range(blocks):
        at = slice(b * BLOCK, (b + 1) * BLOCK)
        pieces = []
        for group in range(2):
            lane = slice(group * 128, group * 128 + 128)
            states = (s1_ref, s2_ref)[group][at, :].astype(F32)
            lead = lead_ref[group * 8 + b : group * 8 + b + 1, :]
            state = (states + jnp.exp(lead) * enter[group]).astype(BF16)
            query = (q1_ref, kq2_ref)[group][at, :]
            row = group * 16 + b
            decay = jnp.where(first, columns[:, row : row + 1], columns[:, row + 8 : row + 9])
            mixer = in_ref[at, lane] + decay * jnp.dot(
                query, state, preferred_element_type=F32
            )
            gated = mixer * silu(gate_ref[at, lane].astype(F32))
            square = gated * gated
            hi = square.astype(BF16)
            low = (square - hi.astype(F32)).astype(BF16)
            mean = (
                jnp.dot(hi, same_head, preferred_element_type=F32)
                + jnp.dot(low, same_head, preferred_element_type=F32)
            ) * (1.0 / 64.0)
            scaled = gated * lax.rsqrt(mean + EPSILON) * gain_ref[group : group + 1, :]
            pieces.append(scaled.astype(BF16))
        to = slice((b % half) * BLOCK, (b % half + 1) * BLOCK)

        @pl.when(c == b // half)
        def _():
            mine_ref[to, 0:128] = pieces[0]
            mine_ref[to, 128:256] = pieces[1]

        @pl.when(c != b // half)
        def _():
            theirs_ref[to, 0:128] = pieces[0]
            theirs_ref[to, 128:256] = pieces[1]


def projection_body(pos_ref, *refs):
    chunk_refs, (w_ref, res_ref, a_ref, b_ref) = refs[:8], refs[8:]
    x, c = pos_ref[0], pos_ref[1]
    total = res_ref[...].astype(F32)
    for j, shift in enumerate((0, -1, 1, 2)):
        there = lax.rem(x + shift + 4, 4)
        for k in range(2):
            who = 2 * there + (c if k == 0 else 1 - c)
            rows = w_ref[pl.ds(pl.multiple_of(who * 256, 256), 256), :]
            total = total + jnp.dot(chunk_refs[2 * j + k][...], rows, preferred_element_type=F32)
    half = a_ref.shape[0]
    a_ref[...] = total[0:half].astype(BF16)
    b_ref[...] = total[half:].astype(BF16)


def mixer_body(
    pos_ref, a0, a1, a2, a3, b0, b1, b2, b3, gain_ref, own_hbm, par_hbm,
    pa0, pa1, pa2, pa3, pb0, pb1, pb2, pb3, w_own, w_par, sems,
):
    x = pos_ref[0]
    width = own_hbm.shape[1] // 3
    copies = []
    for i, (src, dst) in enumerate(((own_hbm, w_own), (par_hbm, w_par))):
        for j, (lo, hi) in enumerate(((0, 2 * width), (2 * width, 3 * width))):
            copy = pltpu.make_async_copy(
                src.at[:, lo:hi], dst.at[:, lo:hi], sems.at[i, j]
            )
            copy.start()
            copies.append(copy)
    starts = [pl.multiple_of(lax.rem(x + s + 4, 4) * 512, 512) for s in (0, -1, 1, 2)]
    contract = (((1,), (1,)), ((), ()))
    waited = set()

    def arrive(i):
        if i not in waited:
            waited.add(i)
            copies[i].wait()

    for ins, outs in (((a0, a1, a2, a3), (pa0, pa1, pa2, pa3)), ((b0, b1, b2, b3), (pb0, pb1, pb2, pb3))):
        wide = [r[...].astype(F32) for r in ins]
        square = sum(jnp.sum(v * v, axis=1, keepdims=True) for v in wide)
        scale = lax.rsqrt(square * (1.0 / 2048.0) + EPSILON)
        normed = [
            (v * scale * gain_ref[0:1, pl.ds(at, 512)]).astype(BF16)
            for v, at in zip(wide, starts)
        ]
        hidden = []
        for i, w in enumerate((w_own, w_par)):
            arrive(2 * i)
            gate = sum(
                jnp.dot(n, w[pl.ds(at, 512), 0:width], preferred_element_type=F32)
                for n, at in zip(normed, starts)
            )
            up = sum(
                jnp.dot(n, w[pl.ds(at, 512), width : 2 * width], preferred_element_type=F32)
                for n, at in zip(normed, starts)
            )
            hidden.append((silu(gate) * up).astype(BF16))
        arrive(1)
        arrive(3)
        for out, at in zip(outs, starts):
            out[...] = (
                lax.dot_general(
                    hidden[0], w_own[pl.ds(at, 512), 2 * width : 3 * width], contract,
                    preferred_element_type=F32,
                )
                + lax.dot_general(
                    hidden[1], w_par[pl.ds(at, 512), 2 * width : 3 * width], contract,
                    preferred_element_type=F32,
                )
            ).astype(BF16)


def last_body(pos_ref, sa, sb, pa, pb, la, lb, ra, rb, mine_ref, theirs_ref):
    c = pos_ref[1]
    half = sa.shape[0]
    for at, s, p, left, right in ((0, sa, pa, la, ra), (half, sb, pb, lb, rb)):
        total = p[...].astype(F32) + left[...].astype(F32) + right[...].astype(F32)
        value = (s[...].astype(F32) + 0.5 * total).astype(BF16)

        @pl.when(c == 0)
        def _():
            mine_ref[at : at + half, :] = value[:, 0:256]
            theirs_ref[at : at + half, :] = value[:, 256:512]

        @pl.when(c == 1)
        def _():
            mine_ref[at : at + half, :] = value[:, 256:512]
            theirs_ref[at : at + half, :] = value[:, 0:256]


def turned(x, axis, distance):
    n = lax.axis_size(axis)
    return lax.ppermute(x, axis, [(i, (i + distance) % n) for i in range(n)])


def along_x(a, b):
    left_a, right_b = turned(a, "x", 1), turned(b, "x", -1)
    left_b, right_a = turned(b, "x", 1), turned(a, "x", -1)
    far_a, far_b = turned(left_a, "x", 1), turned(right_b, "x", -1)
    return (a, left_a, right_a, far_a), (b, left_b, right_b, far_b)


def shards(
    grouped_head_inputs,
    head_gate_inputs,
    unsmoothed_step,
    head_decay_rate,
    extra_log_decay,
    first_group_keys,
    first_group_queries,
    second_group_keys,
    second_group_queries,
    head_input_filter,
    first_group_filter,
    second_group_filter,
    head_norm_gain,
    output_weight,
    residual,
    channel_norm_gain,
    channel_gate_weight,
    channel_up_weight,
    channel_down_weight,
):
    length = grouped_head_inputs.shape[0]
    half = length // 2
    blocks = length // BLOCK
    xi = lax.axis_index("x").astype(jnp.int32)
    ci = lax.axis_index("c").astype(jnp.int32)
    yi = lax.axis_index("y").astype(jnp.int32)
    pos = jnp.stack([xi, ci])
    params = pltpu.CompilerParams(vmem_limit_bytes=56 * 2**20)

    def call(body, outs, args, scratch=(), spaces=None):
        spaces = spaces or [pltpu.VMEM] * len(args)
        return pl.pallas_call(
            body,
            out_shape=outs,
            in_specs=[pl.BlockSpec(memory_space=s) for s in spaces],
            scratch_shapes=list(scratch),
            compiler_params=params,
        )(*args)

    def scalar_first(args):
        return [pltpu.SMEM] + [pltpu.VMEM] * (len(args) - 1)

    own_rows = jnp.concatenate(
        [channel_gate_weight, channel_up_weight, channel_down_weight], axis=1
    )
    own_w = lax.all_gather(own_rows, SP, axis=0, tiled=True)
    x_tail = grouped_head_inputs[-16:].reshape(16, 256)
    k2t, q2t = second_group_keys.T, second_group_queries.T
    packed = pack_rim(x_tail, first_group_keys, first_group_queries, k2t, q2t)
    count = lax.axis_size(SP)
    rim = lax.ppermute(packed, SP, [(i, i + 1) for i in range(count - 1)])
    x_flat = grouped_head_inputs.reshape(length, 256)
    filters = jnp.concatenate(
        [
            head_input_filter.reshape(4, 256),
            first_group_filter.reshape(4, 256),
            second_group_filter.reshape(4, 128),
        ],
        axis=1,
    )
    steps = unsmoothed_step.transpose(1, 2, 0).reshape(4 * blocks, BLOCK)
    extra = extra_log_decay.transpose(1, 2, 0).reshape(4 * blocks, BLOCK)

    args = (
        head_decay_rate, x_flat, first_group_keys, first_group_queries, k2t, q2t, rim, filters,
        steps, extra,
    )
    xc, k1c, q1c, kq2c, cum, soft, s1, s2, lead, end = call(
        states_body,
        (
            shape((length, 256), BF16),
            shape((length, 128), BF16),
            shape((length, 128), BF16),
            shape((length, 128), BF16),
            shape((4 * blocks, BLOCK), F32),
            shape((4 * blocks, BLOCK), F32),
            shape((length, 128), BF16),
            shape((length, 128), BF16),
            shape((16, 128), F32),
            shape((208, 128), BF16),
        ),
        args,
        scratch=(pltpu.VMEM((length + 8, 640), F32),),
        spaces=scalar_first(args),
    )
    output_weight, residual, head_gate_inputs, end = lax.optimization_barrier(
        (output_weight, residual, head_gate_inputs, end)
    )
    before = [turned(end, "y", k) for k in (1, 2, 3)]
    inside = call(inside_body, shape((length, 256), F32), (xc, k1c, q1c, kq2c, cum, soft))
    args = (yi[None], end, *before)
    pre, ylead, total = call(
        combine_body,
        (shape((192, 128), F32), shape((8, 128), F32), shape((208, 128), BF16)),
        args,
        spaces=scalar_first(args),
    )
    rows = lax.axis_size("z")
    earlier = [
        lax.ppermute(total, "z", [(i, i + k) for i in range(rows - k)])
        for k in range(1, rows)
    ]
    gates = head_gate_inputs.reshape(length, 256)
    args = (
        ci[None], inside, gates, q1c, kq2c, cum, s1, s2, lead, head_norm_gain, pre, ylead, *earlier
    )
    mine, theirs = call(
        mixed_body,
        (shape((half, 256), BF16), shape((half, 256), BF16)),
        args,
        spaces=scalar_first(args),
    )
    other = turned(theirs, "c", 1)

    w = output_weight.reshape(2, 8, 128, 256).transpose(1, 0, 2, 3).reshape(2048, 256)
    w_other = turned(w, "c", 1)
    res_other = turned(lax.dynamic_slice_in_dim(residual, (1 - ci) * half, half, axis=0), "c", 1)
    w_both = jnp.where(
        ci == 0, jnp.concatenate([w, w_other], 1), jnp.concatenate([w_other, w], 1)
    )
    res_mine = lax.dynamic_slice_in_dim(residual, ci * half, half, axis=0)
    res_both = jnp.where(
        ci == 0,
        jnp.concatenate([res_mine, res_other], 1),
        jnp.concatenate([res_other, res_mine], 1),
    )

    ours, others = along_x(mine, other)
    args = (pos, *(v for pair in zip(ours, others) for v in pair), w_both, res_both)
    stream_a, stream_b = call(
        projection_body,
        (shape((half // 2, 512), BF16), shape((half // 2, 512), BF16)),
        args,
        spaces=scalar_first(args),
    )
    all_a, all_b = along_x(stream_a, stream_b)
    par_w = turned(lax.optimization_barrier((own_w, all_a[3], all_b[3]))[0], "c", 1)

    args = (pos, *all_a, *all_b, channel_norm_gain[None], own_w, par_w)
    quarter = shape((half // 2, 512), BF16)
    pa0, pa1, pa2, pa3, pb0, pb1, pb2, pb3 = call(
        mixer_body,
        (quarter,) * 8,
        args,
        scratch=(
            pltpu.VMEM(own_w.shape, BF16),
            pltpu.VMEM(own_w.shape, BF16),
            pltpu.SemaphoreType.DMA((2, 2)),
        ),
        spaces=[pltpu.SMEM] + [pltpu.VMEM] * 9 + [pl.ANY] * 2,
    )
    far_a = turned(pa3, "x", 1)
    far_b = turned(pb3, "x", -1)
    left_b = turned(pb2, "x", 1)
    right_a = turned(pa1, "x", -1)
    sum_a = (pa2.astype(F32) + far_a.astype(F32)).astype(BF16)
    sum_b = (pb1.astype(F32) + far_b.astype(F32)).astype(BF16)
    left_a = turned(sum_a, "x", 1)
    right_b = turned(sum_b, "x", -1)
    args = (pos, stream_a, stream_b, pa0, pb0, left_a, left_b, right_a, right_b)
    out_mine, out_theirs = call(
        last_body,
        (shape((half, 256), BF16), shape((half, 256), BF16)),
        args,
        spaces=scalar_first(args),
    )
    out_other = turned(out_theirs, "c", 1)
    return jnp.where(
        ci == 0,
        jnp.concatenate([out_mine, out_other], 0),
        jnp.concatenate([out_other, out_mine], 0),
    )


def solution(mesh):
    sp, tp = mesh.devices.shape
    wide = Mesh(mesh.devices.reshape(sp // 4, 4, tp // 2, 2), ("z", "y", "x", "c"))

    return jax.shard_map(
        shards,
        mesh=wide,
        in_specs=(
            P(SP, None, TP),
            P(SP, None, TP),
            P(SP, None, TP),
            P(None, TP),
            P(SP, None, TP),
            P(SP, None),
            P(SP, None),
            P(SP, None),
            P(SP, None),
            P(None, None, TP),
            P(),
            P(),
            P(None, TP),
            P(None, None, TP),
            P(SP, TP),
            P(),
            P(SP, TP),
            P(SP, TP),
            P(SP, TP),
        ),
        out_specs=P(SP, TP),
        check_vma=False,
    )
```

```python
import jax
import jax.numpy as jnp
from jax import lax
from jax.experimental import pallas as pl
from jax.experimental.pallas import tpu as pltpu
from jax.sharding import Mesh, PartitionSpec as P


EPSILON = 1e-06
BLOCK = 128
F32 = jnp.float32
BF16 = jnp.bfloat16
SP = ("z", "y")
TP = ("x", "c")


def silu(v):
    return v * jax.nn.sigmoid(v)


def shape(dims, kind):
    return jax.ShapeDtypeStruct(dims, kind)


def pack_rim_body(x_ref, k1_ref, q1_ref, k2_ref, q2_ref, out_ref):
    out_ref[:, 0:256] = x_ref[...]
    out_ref[:, 256:384] = k1_ref[...]
    out_ref[:, 384:512] = q1_ref[...]
    both = jnp.concatenate([k2_ref[...], q2_ref[...]], axis=0).astype(F32)
    out_ref[:, 512:640] = both.T[112:128].astype(BF16)


def pack_rim(x_flat, k1, q1, k2t, q2t):
    rows = k1.shape[0] // 16 - 1
    cols = k2t.shape[1] // 128 - 1
    return pl.pallas_call(
        pack_rim_body,
        grid=(1,),
        in_specs=[
            pl.BlockSpec((16, 256), lambda i: (rows, 0)),
            pl.BlockSpec((16, 128), lambda i: (rows, 0)),
            pl.BlockSpec((16, 128), lambda i: (rows, 0)),
            pl.BlockSpec((64, 128), lambda i: (0, cols)),
            pl.BlockSpec((64, 128), lambda i: (0, cols)),
        ],
        out_specs=pl.BlockSpec((16, 640), lambda i: (0, 0)),
        out_shape=shape((16, 640), BF16),
        name="pack_rim",
    )(x_flat, k1, q1, k2t, q2t)


def lanes_of(rows):
    return lax.broadcasted_iota(jnp.int32, (rows, 128), 1) < 64


def three_parts(v):
    hi = v.astype(BF16)
    rest = v - hi.astype(F32)
    mid = rest.astype(BF16)
    low = (rest - mid.astype(F32)).astype(BF16)
    return hi.astype(F32), mid.astype(F32), low.astype(F32)


def states_body(
    rate_ref, x_ref, k1_ref, q1_ref, k2_ref, q2_ref, rim_ref, fx_ref, f1_ref, f2_ref, step_ref,
    extra_ref,
    xc_ref, k1c_ref, q1c_ref, kq2c_ref, cum_ref, sp_ref, s1_ref, s2_ref, lead_ref, end_ref,
    buf, filt, raw, more,
):
    length = x_ref.shape[0]
    blocks = length // BLOCK
    upper = (
        lax.broadcasted_iota(jnp.int32, (BLOCK, BLOCK), 0)
        <= lax.broadcasted_iota(jnp.int32, (BLOCK, BLOCK), 1)
    ).astype(F32)
    raw[...] = jnp.zeros(raw.shape, F32)
    more[...] = jnp.zeros(more.shape, F32)
    for b in range(blocks):
        for head in range(4):
            row = b * 8 + head
            at = slice(b * BLOCK, (b + 1) * BLOCK)
            raw[row : row + 1, :] = step_ref[head // 2, head % 2 : head % 2 + 1, at]
            more[row : row + 1, :] = extra_ref[head // 2, head % 2 : head % 2 + 1, at]
    place = lax.broadcasted_iota(jnp.int32, (8, BLOCK), 0)
    rate = jnp.zeros((8, BLOCK), F32)
    for head in range(4):
        rate = jnp.where(place == head, rate_ref[head // 2, head % 2], rate)
    values = raw[...]
    soft = jnp.maximum(values, 0.0) + jnp.log1p(jnp.exp(-jnp.abs(values)))
    sp_ref[...] = soft
    logs = more[...] - soft * jnp.concatenate([rate] * blocks, axis=0)
    cum_ref[...] = jnp.dot(
        logs, upper, precision=lax.Precision.HIGHEST, preferred_element_type=F32
    )
    for k in range(4):
        filt[k : k + 1, 0:128] = fx_ref[k, 0:1, :]
        filt[k : k + 1, 128:256] = fx_ref[k, 1:2, :]
        filt[k : k + 1, 256:384] = f1_ref[k, 0:1, :]
        filt[k : k + 1, 384:512] = f1_ref[k, 1:2, :]
        filt[k : k + 1, 512:640] = jnp.concatenate([f2_ref[k, 0:1, :], f2_ref[k, 1:2, :]], axis=1)
    buf[0:8, :] = rim_ref[8:16, :].astype(F32)
    first = lanes_of(1)

    def fill(b, none):
        at = pl.ds(pl.multiple_of(b * BLOCK, BLOCK), BLOCK)
        to = pl.ds(pl.multiple_of(b * BLOCK + 8, 8), BLOCK)
        buf[to, 0:256] = x_ref[at, :].astype(F32)
        buf[to, 256:384] = k1_ref[at, :].astype(F32)
        buf[to, 384:512] = q1_ref[at, :].astype(F32)
        both = jnp.concatenate([k2_ref[:, at], q2_ref[:, at]], axis=0).astype(F32)
        buf[to, 512:640] = both.T
        return none

    def step(b, carry):
        state_one, state_two, lead_one, lead_two = carry
        fill(b, 0)
        at = pl.ds(pl.multiple_of(b * BLOCK, BLOCK), BLOCK)
        around = pl.ds(pl.multiple_of(b * BLOCK, BLOCK), BLOCK + 8)

        def conv(lo, hi):
            window = buf[around, lo:hi]
            run = filt[0:1, lo:hi] * window[5 : 5 + BLOCK]
            for k in range(1, 4):
                run = run + filt[k : k + 1, lo:hi] * window[5 + k : 5 + k + BLOCK]
            return silu(run)

        x_one = conv(0, 128).astype(BF16)
        x_two = conv(128, 256).astype(BF16)
        xc_ref[at, 0:128] = x_one
        xc_ref[at, 128:256] = x_two
        k_one = conv(256, 384)
        k1c_ref[at, :] = k_one.astype(BF16)
        q1c_ref[at, :] = conv(384, 512).astype(BF16)
        kq_two = conv(512, 640)
        kq2c_ref[at, :] = kq_two.astype(BF16)
        s1_ref[at, :] = state_one.astype(BF16)
        s2_ref[at, :] = jnp.concatenate(
            [jnp.zeros((64, 128), BF16), state_two.astype(BF16)], axis=0
        )
        eight = pl.ds(pl.multiple_of(b * 8, 8), 8)
        lead_ref[eight, :] = jnp.concatenate(
            [lead_one, lead_two, jnp.zeros((6, 128), F32)], axis=0
        )
        rows, softs = cum_ref[eight, :], sp_ref[eight, :]
        tot = rows[:, 127:128]
        weight = jnp.exp(tot - rows) * softs
        key_one = k_one.T
        key_two = kq_two.T[0:64]
        ups = [
            jnp.dot(
                ((key_one if head < 2 else key_two) * weight[head : head + 1, :]).astype(BF16),
                x_one if head < 2 else x_two,
                preferred_element_type=F32,
            )
            for head in range(4)
        ]
        wide = jnp.broadcast_to(tot, (8, 128))
        tot_one = jnp.where(first, wide[0:1], wide[1:2])
        tot_two = jnp.where(first, wide[2:3], wide[3:4])
        return (
            state_one * jnp.exp(tot_one) + jnp.where(first, ups[0], ups[1]),
            state_two * jnp.exp(tot_two) + jnp.where(first, ups[2], ups[3]),
            lead_one + tot_one,
            lead_two + tot_two,
        )

    state_one, state_two, lead_one, lead_two = lax.fori_loop(
        0,
        blocks,
        step,
        (
            jnp.zeros((128, 128), F32),
            jnp.zeros((64, 128), F32),
            jnp.zeros((1, 128), F32),
            jnp.zeros((1, 128), F32),
        ),
    )
    end_ref[0:128, :] = state_one.astype(BF16)
    end_ref[128:192, :] = state_two.astype(BF16)
    end_ref[192:208, :] = log_rows(lead_one, lead_two)


def log_rows(one, two):
    parts = three_parts(one) + three_parts(two)
    return jnp.concatenate(list(parts) + [jnp.zeros((10, 128), F32)], axis=0).astype(BF16)


def logs_in(payload_ref):
    rows = payload_ref[192:208, :].astype(F32)
    one = rows[0:1] + rows[1:2] + rows[2:3]
    two = rows[3:4] + rows[4:5] + rows[5:6]
    return one, two


def inside_body(xc_ref, k1_ref, q1_ref, kq2_ref, cum_ref, sp_ref, out_ref):
    length = xc_ref.shape[0]
    causal = lax.broadcasted_iota(jnp.int32, (BLOCK, BLOCK), 0) >= lax.broadcasted_iota(
        jnp.int32, (BLOCK, BLOCK), 1
    )
    first = lanes_of(1)
    contract = (((1,), (1,)), ((), ()))

    def step(b, none):
        at = pl.ds(pl.multiple_of(b * BLOCK, BLOCK), BLOCK)
        eight = pl.ds(pl.multiple_of(b * 8, 8), 8)
        rows, softs = cum_ref[eight, :], sp_ref[eight, :]
        columns = rows.T
        kq_two = kq2_ref[at, :].astype(F32)
        query_two = jnp.where(first, 0.0, kq_two).astype(BF16)
        key_two = pltpu.roll(kq_two, 64, 1).astype(BF16)
        scores = (
            lax.dot_general(q1_ref[at, :], k1_ref[at, :], contract, preferred_element_type=F32),
            lax.dot_general(query_two, key_two, contract, preferred_element_type=F32),
        )
        for group in range(2):
            values = xc_ref[at, group * 128 : group * 128 + 128]
            parts = []
            for inner in range(2):
                h = group * 2 + inner
                spans = jnp.where(causal, columns[:, h : h + 1] - rows[h : h + 1, :], -jnp.inf)
                weights = jnp.exp(spans) * (scores[group] * softs[h : h + 1, :])
                parts.append(jnp.dot(weights.astype(BF16), values, preferred_element_type=F32))
            out_ref[at, group * 128 : group * 128 + 128] = jnp.where(first, parts[0], parts[1])
        return none

    lax.fori_loop(0, length // BLOCK, step, 0)


def combine_body(y_ref, own_ref, b1_ref, b2_ref, b3_ref, pre_ref, lead_ref, total_ref):
    y = y_ref[3]
    refs = (own_ref, b1_ref, b2_ref, b3_ref)
    place = [lax.rem(y - k + 4, 4) for k in range(4)]
    logs = [logs_in(r) for r in refs]
    zero = jnp.zeros((1, 128), F32)

    def pick(flag, v):
        return jnp.where(flag, v, zero)

    leads = [zero, zero]
    pre_one = jnp.zeros((128, 128), F32)
    pre_two = jnp.zeros((64, 128), F32)
    tot_one = jnp.zeros((128, 128), F32)
    tot_two = jnp.zeros((64, 128), F32)
    for k in range(4):
        one = refs[k][0:128, :].astype(F32)
        two = refs[k][128:192, :].astype(F32)
        if k:
            flag = k <= y
            pre_one = pre_one + pick(flag, jnp.exp(leads[0])) * one
            pre_two = pre_two + pick(flag, jnp.exp(leads[1])) * two
            leads = [leads[g] + pick(flag, logs[k][g]) for g in range(2)]
        later = [zero, zero]
        for j in range(4):
            if j != k:
                flag = place[j] > place[k]
                later = [later[g] + pick(flag, logs[j][g]) for g in range(2)]
        tot_one = tot_one + jnp.exp(later[0]) * one
        tot_two = tot_two + jnp.exp(later[1]) * two
    pre_ref[0:128, :] = pre_one
    pre_ref[128:192, :] = pre_two
    lead_ref[0:1, :] = leads[0]
    lead_ref[1:2, :] = leads[1]
    tot_one = tot_one.astype(BF16)
    tot_two = tot_two.astype(BF16)
    tot_logs = log_rows(
        logs[0][0] + logs[1][0] + logs[2][0] + logs[3][0],
        logs[0][1] + logs[1][1] + logs[2][1] + logs[3][1],
    )
    for z in range(total_ref.shape[0]):
        total_ref[z, 0:128, :] = tot_one
        total_ref[z, 128:192, :] = tot_two
        total_ref[z, 192:208, :] = tot_logs


def mixed_body(
    pos_ref, in_ref, gate_ref, q1_ref, kq2_ref, cum_ref, s1_ref, s2_ref, lead_ref, gain_ref,
    pre_ref, ylead_ref, rows_ref, mine_ref, theirs_ref,
):
    c, z = pos_ref[1], pos_ref[2]
    far_one = jnp.zeros((128, 128), F32)
    far_two = jnp.zeros((64, 128), F32)
    run = [jnp.zeros((1, 128), F32)] * 2
    for k in reversed(range(rows_ref.shape[0] - 1)):
        flag = k < z
        r = rows_ref.at[k]
        scale = [jnp.where(flag, jnp.exp(v), 0.0) for v in run]
        far_one = far_one + scale[0] * r[0:128, :].astype(F32)
        far_two = far_two + scale[1] * r[128:192, :].astype(F32)
        logs = logs_in(r)
        run = [v + jnp.where(flag, more, 0.0) for v, more in zip(run, logs)]
    enter = (
        pre_ref[0:128, :] + jnp.exp(ylead_ref[0:1, :]) * far_one,
        jnp.concatenate(
            [
                jnp.zeros((64, 128), F32),
                pre_ref[128:192, :] + jnp.exp(ylead_ref[1:2, :]) * far_two,
            ],
            axis=0,
        ),
    )
    first = lanes_of(1)
    same_head = (
        (lax.broadcasted_iota(jnp.int32, (128, 128), 0) < 64)
        == (lax.broadcasted_iota(jnp.int32, (128, 128), 1) < 64)
    ).astype(BF16)
    blocks = in_ref.shape[0] // BLOCK
    half = blocks // 2

    def block(b, out_ref, to):
        at = pl.ds(pl.multiple_of(b * BLOCK, BLOCK), BLOCK)
        eight = pl.ds(pl.multiple_of(b * 8, 8), 8)
        columns = jnp.exp(cum_ref[eight, :].T)
        leads = jnp.exp(lead_ref[eight, :])
        for group in range(2):
            lane = slice(group * 128, group * 128 + 128)
            states = (s1_ref, s2_ref)[group][at, :].astype(F32)
            state = (states + leads[group : group + 1, :] * enter[group]).astype(BF16)
            query = (q1_ref, kq2_ref)[group][at, :]
            h = group * 2
            decay = jnp.where(first, columns[:, h : h + 1], columns[:, h + 1 : h + 2])
            mixer = in_ref[at, lane] + decay * jnp.dot(
                query, state, preferred_element_type=F32
            )
            gated = mixer * silu(gate_ref[at, lane].astype(F32))
            square = gated * gated
            hi = square.astype(BF16)
            low = (square - hi.astype(F32)).astype(BF16)
            mean = (
                jnp.dot(hi, same_head, preferred_element_type=F32)
                + jnp.dot(low, same_head, preferred_element_type=F32)
            ) * (1.0 / 64.0)
            scaled = gated * lax.rsqrt(mean + EPSILON) * gain_ref[group : group + 1, :]
            out_ref[to, lane] = scaled.astype(BF16)

    def step(i, none):
        to = pl.ds(pl.multiple_of(i * BLOCK, BLOCK), BLOCK)
        block(c * half + i, mine_ref, to)
        block((1 - c) * half + i, theirs_ref, to)
        return none

    lax.fori_loop(0, half, step, 0)


def projection_body(pos_ref, *refs):
    chunk_refs, (w_ref, res_ref, a_ref, b_ref, lhs) = refs[:8], refs[8:]
    x, c = pos_ref[0], pos_ref[1]
    for j, shift in enumerate((0, -1, 1, 2)):
        there = lax.rem(x + shift + 4, 4)
        for k in range(2):
            who = 2 * there + (c if k == 0 else 1 - c)
            lhs[:, pl.ds(pl.multiple_of(who * 256, 256), 256)] = chunk_refs[2 * j + k][...]
    total = res_ref[...].astype(F32) + jnp.dot(
        lhs[...], w_ref[...], preferred_element_type=F32
    )
    half = a_ref.shape[0]
    a_ref[...] = total[0:half].astype(BF16)
    b_ref[...] = total[half:].astype(BF16)


def normed_body(pos_ref, *refs):
    ins, gain_ref, out_ref = refs[:8], refs[8], refs[9]
    size = ins[0].shape[0]
    for k in range(2):
        full = [r[...].astype(F32) for r in ins[4 * k : 4 * k + 4]]
        square = sum(jnp.sum(v * v, axis=1, keepdims=True) for v in full)
        scale = lax.rsqrt(square * (1.0 / 2048.0) + EPSILON)
        for v, shift in zip(full, SHIFTS):
            at = lax.rem(pos_ref[0] + shift + 4, 4)
            lanes = pl.ds(pl.multiple_of(at * 512, 512), 512)
            out_ref[k * size : (k + 1) * size, lanes] = (v * scale * gain_ref[0:1, lanes]).astype(
                BF16
            )


def hidden_chunk(normed, wide_ref, hidden, lanes, width):
    depth = wide_ref.shape[1] * wide_ref.shape[2]
    gate, up = (
        jnp.dot(
            normed[...], wide_ref[part, :, :, lanes].reshape(depth, width),
            preferred_element_type=F32,
        )
        for part in range(2)
    )
    hidden[:, lanes] = (silu(gate) * up).astype(BF16)


def down_part(hidden, down, at, out_a, out_b):
    tall = down.shape[0] // 4
    rows = down[pl.ds(at * tall, tall), :, :].reshape(tall * down.shape[1], down.shape[2])
    contract = (((1,), (1,)), ((), ()))
    part = lax.dot_general(hidden[...], rows, contract, preferred_element_type=F32).astype(BF16)
    half = part.shape[0] // 2
    out_a[...] = part[0:half]
    out_b[...] = part[half:]


SHIFTS = (0, -1, 1, 2)
FAR_FIRST = (3, 1, 2, 0)
AHEAD = 9


def hidden_body(
    pos_ref, normed, w_hbm, far_a, far_b, hidden, down, w_ref, sems, down_sems
):
    x = pos_ref[0]
    width = w_hbm.shape[3] // 3
    groups = w_hbm.shape[0]
    tall = groups // 4
    whole = width // 256
    rest = width - whole * 256
    chunks = 2 * whole
    last = chunks * 256
    starts = [lax.rem(x + s + 4, 4) for s in SHIFTS]

    def pieces(n):
        for part in range(2):
            for k in range(2):
                rows = pl.ds(k * (groups // 2), groups // 2)
                to = w_ref.at[part]
                if n == chunks:
                    for i in range(2):
                        yield pltpu.make_async_copy(
                            w_hbm.at[rows, i, :, part * width + whole * 256 : (part + 1) * width],
                            to.at[rows, :, last + i * rest : last + (i + 1) * rest],
                            sems.at[n, part, 2 * k + i],
                        )
                else:
                    at = part * width + (n % whole) * 256
                    yield pltpu.make_async_copy(
                        w_hbm.at[rows, n // whole, :, at : at + 256],
                        to.at[rows, :, n * 256 : (n + 1) * 256],
                        sems.at[n, part, k],
                    )

    def down_pieces(j):
        rows = pl.ds(starts[j] * tall, tall)
        for i in range(2):
            for k, (lo, hi, to) in enumerate(
                ((0, whole * 256, i * whole * 256), (whole * 256, width, last + i * rest))
            ):
                yield pltpu.make_async_copy(
                    w_hbm.at[rows, i, :, 2 * width + lo : 2 * width + hi],
                    down.at[rows, :, to : to + hi - lo],
                    down_sems.at[j, i, k],
                )

    def begin(copies):
        for each in copies:
            each.start()

    def finish(copies):
        for each in copies:
            each.wait()

    order = [pieces(n) for n in range(chunks + 1)]
    order = [list(each) for each in order] + [list(down_pieces(j)) for j in FAR_FIRST]
    for each in order[:AHEAD]:
        begin(each)
    for n in range(chunks + 1):
        finish(order[n])
        if n + AHEAD < len(order):
            begin(order[n + AHEAD])
        wide = 256 if n < chunks else 2 * rest
        hidden_chunk(normed, w_ref, hidden, slice(n * 256, n * 256 + wide), wide)
    for each in order[chunks + 1 + AHEAD :]:
        begin(each)
    finish(down_pieces(FAR_FIRST[0]))
    down_part(hidden, down, starts[FAR_FIRST[0]], far_a, far_b)
    for j in FAR_FIRST[1:]:
        finish(down_pieces(j))


def near_body(pos_ref, hidden, down, *outs):
    for k, j in enumerate(FAR_FIRST[1:]):
        at = lax.rem(pos_ref[0] + SHIFTS[j] + 4, 4)
        down_part(hidden, down, at, outs[2 * k], outs[2 * k + 1])


def last_body(
    pos_ref, sa_ref, pa_ref, la_ref, ra_ref, sb_ref, pb_ref, lb_ref, rb_ref, mine_ref, theirs_ref
):
    c = pos_ref[1]
    size = sa_ref.shape[0]
    parts = ((sa_ref, pa_ref, la_ref, ra_ref), (sb_ref, pb_ref, lb_ref, rb_ref))
    for k, (s_ref, p_ref, left_ref, right_ref) in enumerate(parts):
        at = slice(k * size, (k + 1) * size)
        for ref, who in ((theirs_ref, 1 - c), (mine_ref, c)):
            lanes = pl.ds(pl.multiple_of(who * 256, 256), 256)
            total = (
                p_ref[:, lanes].astype(F32)
                + left_ref[:, lanes].astype(F32)
                + right_ref[:, lanes].astype(F32)
            )
            ref[at, :] = (s_ref[:, lanes].astype(F32) + 0.5 * total).astype(BF16)


def join_body(pos_ref, mine_ref, other_ref, out_ref, sems):
    c = pos_ref[1]
    size = mine_ref.shape[0]
    copies = []
    for k, (half, ref) in enumerate(((c, mine_ref), (1 - c, other_ref))):
        at = pl.ds(pl.multiple_of(half * size, size), size)
        copies.append(pltpu.make_async_copy(ref, out_ref.at[at, :], sems.at[k]))
    for each in copies:
        each.start()
    for each in copies:
        each.wait()


def turned(x, axis, distance):
    n = lax.axis_size(axis)
    return lax.ppermute(x, axis, [(i, (i + distance) % n) for i in range(n)])


def along_x(a, b):
    left_a, right_b = turned(a, "x", 1), turned(b, "x", -1)
    left_b, right_a = turned(b, "x", 1), turned(a, "x", -1)
    far_a, far_b = turned(left_a, "x", 1), turned(right_b, "x", -1)
    return (a, left_a, right_a, far_a), (b, left_b, right_b, far_b)


def shards(
    grouped_head_inputs,
    head_gate_inputs,
    unsmoothed_step,
    head_decay_rate,
    extra_log_decay,
    first_group_keys,
    first_group_queries,
    second_group_keys,
    second_group_queries,
    head_input_filter,
    first_group_filter,
    second_group_filter,
    head_norm_gain,
    output_weight,
    residual,
    channel_norm_gain,
    channel_gate_weight,
    channel_up_weight,
    channel_down_weight,
):
    length = grouped_head_inputs.shape[0]
    half = length // 2
    blocks = length // BLOCK
    xi = lax.axis_index("x").astype(jnp.int32)
    ci = lax.axis_index("c").astype(jnp.int32)
    yi = lax.axis_index("y").astype(jnp.int32)
    zi = lax.axis_index("z").astype(jnp.int32)
    pos = jnp.stack([xi, ci, zi, yi])

    def call(body, outs, args, name, scratch=(), spaces=None, limit=12, flops=None, loose=(), spilled=()):
        spaces = spaces or [pltpu.VMEM] * len(args)
        single = not isinstance(outs, tuple)
        outs = (outs,) if single else outs
        args = [
            a
            if s is pltpu.SMEM
            else pltpu.with_memory_space_constraint(a, pltpu.HBM if i in loose else s)
            for i, (a, s) in enumerate(zip(args, spaces))
        ]
        done = pl.pallas_call(
            body,
            out_shape=tuple(
                (pltpu.HBM if i in spilled else pltpu.VMEM)(o.shape, o.dtype)
                for i, o in enumerate(outs)
            ),
            in_specs=[pl.BlockSpec(memory_space=s) for s in spaces],
            out_specs=tuple(
                pl.BlockSpec(memory_space=pltpu.HBM if name == "join" else pltpu.VMEM)
                for _ in outs
            ),
            scratch_shapes=list(scratch),
            cost_estimate=flops
            and pl.CostEstimate(flops=flops, transcendentals=0, bytes_accessed=10**6),
            compiler_params=pltpu.CompilerParams(vmem_limit_bytes=limit * 2**20),
        )(*args)
        return done[0] if single else done

    def scalar_first(args):
        return [pltpu.SMEM] + [pltpu.VMEM] * (len(args) - 1)

    own_rows = jnp.concatenate(
        [channel_gate_weight, channel_up_weight, channel_down_weight], axis=1
    )
    all_w = lax.all_gather(own_rows, SP + ("c",), axis=0, tiled=True)
    x_flat = grouped_head_inputs.reshape(length, 256)
    k2t, q2t = second_group_keys.T, second_group_queries.T
    packed = pack_rim(x_flat, first_group_keys, first_group_queries, k2t, q2t)
    count = lax.axis_size(SP)
    rim = lax.ppermute(packed, SP, [(i, i + 1) for i in range(count - 1)])

    args = (
        head_decay_rate, x_flat, first_group_keys, first_group_queries, k2t, q2t, rim,
        head_input_filter, first_group_filter, second_group_filter,
        unsmoothed_step.transpose(1, 2, 0), extra_log_decay.transpose(1, 2, 0),
    )
    xc, k1c, q1c, kq2c, cum, soft, s1, s2, lead, end = call(
        states_body,
        (
            shape((length, 256), BF16),
            shape((length, 128), BF16),
            shape((length, 128), BF16),
            shape((length, 128), BF16),
            shape((8 * blocks, BLOCK), F32),
            shape((8 * blocks, BLOCK), F32),
            shape((length, 128), BF16),
            shape((length, 128), BF16),
            shape((8 * blocks, 128), F32),
            shape((208, 128), BF16),
        ),
        args,
        "states",
        loose=(1, 2, 3, 4, 5, 7, 8, 9, 10, 11),
        spilled=(1, 6, 7),
        scratch=(
            pltpu.VMEM((length + 8, 640), F32),
            pltpu.VMEM((8, 640), F32),
            pltpu.VMEM((8 * blocks, BLOCK), F32),
            pltpu.VMEM((8 * blocks, BLOCK), F32),
        ),
        spaces=scalar_first(args),
    )
    output_weight, residual, head_gate_inputs, end = lax.optimization_barrier(
        (output_weight, residual, head_gate_inputs, end)
    )
    before = [turned(end, "y", k) for k in (1, 2, 3)]
    args = (pos, end, *before)
    pre, ylead, total = call(
        combine_body,
        (shape((192, 128), F32), shape((8, 128), F32), shape((lax.axis_size("z"), 208, 128), BF16)),
        args,
        "combine",
        spaces=scalar_first(args),
    )
    rows = lax.all_to_all(total, "z", 0, 0, tiled=True)
    xc = lax.optimization_barrier((xc, total))[0]
    inside = call(
        inside_body,
        shape((length, 256), F32),
        (xc, k1c, q1c, kq2c, cum, soft),
        "inside",
        loose=(1,),
    )
    gates = head_gate_inputs.reshape(length, 256)
    args = (
        pos, inside, gates, q1c, kq2c, cum, s1, s2, lead, head_norm_gain, pre, ylead, rows
    )
    mine, theirs = call(
        mixed_body,
        (shape((half, 256), BF16), shape((half, 256), BF16)),
        args,
        "mixed",
        loose=(2, 6, 7, 9),
        spaces=scalar_first(args),
    )
    other = turned(theirs, "c", 1)

    w = output_weight.reshape(2, 8, 128, 256).transpose(1, 0, 2, 3).reshape(2048, 256)
    w_other = turned(w, "c", 1)
    res_other = turned(lax.dynamic_slice_in_dim(residual, (1 - ci) * half, half, axis=0), "c", 1)
    w_both = jnp.where(
        ci == 0, jnp.concatenate([w, w_other], 1), jnp.concatenate([w_other, w], 1)
    )
    res_mine = lax.dynamic_slice_in_dim(residual, ci * half, half, axis=0)
    res_both = jnp.where(
        ci == 0,
        jnp.concatenate([res_mine, res_other], 1),
        jnp.concatenate([res_other, res_mine], 1),
    )

    ours, others = along_x(mine, other)
    args = (pos, *(v for pair in zip(ours, others) for v in pair), w_both, res_both)
    stream_a, stream_b = call(
        projection_body,
        (shape((half // 2, 512), BF16), shape((half // 2, 512), BF16)),
        args,
        "projection",
        scratch=(pltpu.VMEM((half, 2048), BF16),),
        spaces=scalar_first(args),
    )
    all_a, all_b = along_x(stream_a, stream_b)
    quarter = shape((half // 2, 512), BF16)
    shard_rows, shard_cols = own_rows.shape
    all_w = all_w.reshape(-1, 2, shard_rows, shard_cols)
    wide = (all_w.shape[0], shard_rows, shard_cols // 3 * 2)

    normed = call(
        normed_body,
        shape((half, 2048), BF16),
        (pos, *all_a, *all_b, channel_norm_gain[None]),
        "normed",
        loose=(9,),
        spaces=[pltpu.SMEM] + [pltpu.VMEM] * 9,
    )
    pa3, pb3, hidden, down = call(
        hidden_body,
        (quarter, quarter, shape((half, wide[2]), BF16), shape(wide, BF16)),
        (pos, normed, all_w),
        "hidden",
        scratch=(
            pltpu.VMEM((2, *wide), BF16),
            pltpu.SemaphoreType.DMA((shard_cols // 3 // 256 * 2 + 1, 2, 4)),
            pltpu.SemaphoreType.DMA((4, 2, 2)),
        ),
        spaces=[pltpu.SMEM, pltpu.VMEM, pltpu.HBM],
        limit=20,
    )
    far_a = turned(pa3, "x", 1)
    far_b = turned(pb3, "x", -1)
    pa1, pb1, pa2, pb2, pa0, pb0 = call(
        near_body,
        (quarter,) * 6,
        (pos, hidden, down),
        "near",
        spaces=[pltpu.SMEM] + [pltpu.VMEM] * 2,
    )
    left_b = turned(pb2, "x", 1)
    right_a = turned(pa1, "x", -1)
    sum_a = (pa2.astype(F32) + far_a.astype(F32)).astype(BF16)
    left_a = turned(sum_a, "x", 1)
    sum_b = (pb1.astype(F32) + far_b.astype(F32)).astype(BF16)
    right_b = turned(sum_b, "x", -1)
    mine, theirs = call(
        last_body,
        (shape((half, 256), BF16),) * 2,
        (pos, stream_a, pa0, left_a, right_a, stream_b, pb0, left_b, right_b),
        "last",
        spaces=[pltpu.SMEM] + [pltpu.VMEM] * 8,
    )
    other = turned(theirs, "c", 1)
    return call(
        join_body,
        shape((length, 256), BF16),
        (pos, mine, other),
        "join",
        spilled=(0,),
        scratch=(pltpu.SemaphoreType.DMA((2,)),),
        spaces=[pltpu.SMEM] + [pltpu.VMEM] * 2,
    )


def solution(mesh):
    sp, tp = mesh.devices.shape
    wide = Mesh(mesh.devices.reshape(sp // 4, 4, tp // 2, 2), ("z", "y", "x", "c"))

    return jax.shard_map(
        shards,
        mesh=wide,
        in_specs=(
            P(SP, None, TP),
            P(SP, None, TP),
            P(SP, None, TP),
            P(None, TP),
            P(SP, None, TP),
            P(SP, None),
            P(SP, None),
            P(SP, None),
            P(SP, None),
            P(None, None, TP),
            P(),
            P(),
            P(None, TP),
            P(None, None, TP),
            P(SP, TP),
            P(),
            P(SP, TP),
            P(SP, TP),
            P(SP, TP),
        ),
        out_specs=P(SP, TP),
        check_vma=False,
    )
```

```python
import jax
import jax.numpy as jnp
from jax import lax
from jax.experimental import pallas as pl
from jax.experimental.pallas import tpu as pltpu
from jax.sharding import Mesh, PartitionSpec as P


EPSILON = 1e-06
BLOCK = 128
F32 = jnp.float32
BF16 = jnp.bfloat16
SP = ("z", "y")
TP = ("x", "c")


def silu(v):
    return v * jax.nn.sigmoid(v)


def shape(dims, kind):
    return jax.ShapeDtypeStruct(dims, kind)


def pack_rim_body(x_ref, k1_ref, q1_ref, k2_ref, q2_ref, out_ref):
    out_ref[:, 0:256] = x_ref[...]
    out_ref[:, 256:384] = k1_ref[...]
    out_ref[:, 384:512] = q1_ref[...]
    both = jnp.concatenate([k2_ref[...], q2_ref[...]], axis=0).astype(F32)
    out_ref[:, 512:640] = both.T[112:128].astype(BF16)


def pack_rim(x_flat, k1, q1, k2t, q2t):
    rows = k1.shape[0] // 16 - 1
    cols = k2t.shape[1] // 128 - 1
    return pl.pallas_call(
        pack_rim_body,
        grid=(1,),
        in_specs=[
            pl.BlockSpec((16, 256), lambda i: (rows, 0)),
            pl.BlockSpec((16, 128), lambda i: (rows, 0)),
            pl.BlockSpec((16, 128), lambda i: (rows, 0)),
            pl.BlockSpec((64, 128), lambda i: (0, cols)),
            pl.BlockSpec((64, 128), lambda i: (0, cols)),
        ],
        out_specs=pl.BlockSpec((16, 640), lambda i: (0, 0)),
        out_shape=shape((16, 640), BF16),
        name="pack_rim",
    )(x_flat, k1, q1, k2t, q2t)


def lanes_of(rows):
    return lax.broadcasted_iota(jnp.int32, (rows, 128), 1) < 64


def three_parts(v):
    hi = v.astype(BF16)
    rest = v - hi.astype(F32)
    mid = rest.astype(BF16)
    low = (rest - mid.astype(F32)).astype(BF16)
    return hi.astype(F32), mid.astype(F32), low.astype(F32)


def states_body(
    rate_ref, x_ref, k1_ref, q1_ref, k2_ref, q2_ref, rim_ref, fx_ref, f1_ref, f2_ref, step_ref,
    extra_ref,
    xc_ref, k1c_ref, q1c_ref, kq2c_ref, cum_ref, sp_ref, s1_ref, s2_ref, lead_ref, end_ref,
    buf, filt, raw, more,
):
    length = x_ref.shape[0]
    blocks = length // BLOCK
    upper = (
        lax.broadcasted_iota(jnp.int32, (BLOCK, BLOCK), 0)
        <= lax.broadcasted_iota(jnp.int32, (BLOCK, BLOCK), 1)
    ).astype(F32)
    raw[...] = jnp.zeros(raw.shape, F32)
    more[...] = jnp.zeros(more.shape, F32)
    for b in range(blocks):
        for head in range(4):
            row = b * 8 + head
            at = slice(b * BLOCK, (b + 1) * BLOCK)
            raw[row : row + 1, :] = step_ref[head // 2, head % 2 : head % 2 + 1, at]
            more[row : row + 1, :] = extra_ref[head // 2, head % 2 : head % 2 + 1, at]
    place = lax.broadcasted_iota(jnp.int32, (8, BLOCK), 0)
    rate = jnp.zeros((8, BLOCK), F32)
    for head in range(4):
        rate = jnp.where(place == head, rate_ref[head // 2, head % 2], rate)
    values = raw[...]
    soft = jnp.maximum(values, 0.0) + jnp.log1p(jnp.exp(-jnp.abs(values)))
    sp_ref[...] = soft
    logs = more[...] - soft * jnp.concatenate([rate] * blocks, axis=0)
    cum_ref[...] = jnp.dot(
        logs, upper, precision=lax.Precision.HIGHEST, preferred_element_type=F32
    )
    for k in range(4):
        filt[k : k + 1, 0:128] = fx_ref[k, 0:1, :]
        filt[k : k + 1, 128:256] = fx_ref[k, 1:2, :]
        filt[k : k + 1, 256:384] = f1_ref[k, 0:1, :]
        filt[k : k + 1, 384:512] = f1_ref[k, 1:2, :]
        filt[k : k + 1, 512:640] = jnp.concatenate([f2_ref[k, 0:1, :], f2_ref[k, 1:2, :]], axis=1)
    buf[0:8, :] = rim_ref[8:16, :].astype(F32)
    first = lanes_of(1)

    def fill(b, none):
        at = pl.ds(pl.multiple_of(b * BLOCK, BLOCK), BLOCK)
        to = pl.ds(pl.multiple_of(b * BLOCK + 8, 8), BLOCK)
        buf[to, 0:256] = x_ref[at, :].astype(F32)
        buf[to, 256:384] = k1_ref[at, :].astype(F32)
        buf[to, 384:512] = q1_ref[at, :].astype(F32)
        both = jnp.concatenate([k2_ref[:, at], q2_ref[:, at]], axis=0).astype(F32)
        buf[to, 512:640] = both.T
        return none

    def step(b, carry):
        state_one, state_two, lead_one, lead_two = carry
        fill(b, 0)
        at = pl.ds(pl.multiple_of(b * BLOCK, BLOCK), BLOCK)
        around = pl.ds(pl.multiple_of(b * BLOCK, BLOCK), BLOCK + 8)

        def conv(lo, hi):
            window = buf[around, lo:hi]
            run = filt[0:1, lo:hi] * window[5 : 5 + BLOCK]
            for k in range(1, 4):
                run = run + filt[k : k + 1, lo:hi] * window[5 + k : 5 + k + BLOCK]
            return silu(run)

        x_one = conv(0, 128).astype(BF16)
        x_two = conv(128, 256).astype(BF16)
        xc_ref[at, 0:128] = x_one
        xc_ref[at, 128:256] = x_two
        k_one = conv(256, 384)
        k1c_ref[at, :] = k_one.astype(BF16)
        q1c_ref[at, :] = conv(384, 512).astype(BF16)
        kq_two = conv(512, 640)
        kq2c_ref[at, :] = kq_two.astype(BF16)
        s1_ref[at, :] = state_one.astype(BF16)
        s2_ref[at, :] = jnp.concatenate(
            [jnp.zeros((64, 128), BF16), state_two.astype(BF16)], axis=0
        )
        eight = pl.ds(pl.multiple_of(b * 8, 8), 8)
        lead_ref[eight, :] = jnp.concatenate(
            [lead_one, lead_two, jnp.zeros((6, 128), F32)], axis=0
        )
        rows, softs = cum_ref[eight, :], sp_ref[eight, :]
        tot = rows[:, 127:128]
        weight = jnp.exp(tot - rows) * softs
        key_one = k_one.T
        key_two = kq_two.T[0:64]
        ups = [
            jnp.dot(
                ((key_one if head < 2 else key_two) * weight[head : head + 1, :]).astype(BF16),
                x_one if head < 2 else x_two,
                preferred_element_type=F32,
            )
            for head in range(4)
        ]
        wide = jnp.broadcast_to(tot, (8, 128))
        tot_one = jnp.where(first, wide[0:1], wide[1:2])
        tot_two = jnp.where(first, wide[2:3], wide[3:4])
        return (
            state_one * jnp.exp(tot_one) + jnp.where(first, ups[0], ups[1]),
            state_two * jnp.exp(tot_two) + jnp.where(first, ups[2], ups[3]),
            lead_one + tot_one,
            lead_two + tot_two,
        )

    state_one, state_two, lead_one, lead_two = lax.fori_loop(
        0,
        blocks,
        step,
        (
            jnp.zeros((128, 128), F32),
            jnp.zeros((64, 128), F32),
            jnp.zeros((1, 128), F32),
            jnp.zeros((1, 128), F32),
        ),
    )
    end_ref[0:128, :] = state_one.astype(BF16)
    end_ref[128:192, :] = state_two.astype(BF16)
    end_ref[192:208, :] = log_rows(lead_one, lead_two)


def log_rows(one, two):
    parts = three_parts(one) + three_parts(two)
    return jnp.concatenate(list(parts) + [jnp.zeros((10, 128), F32)], axis=0).astype(BF16)


def logs_in(payload_ref):
    rows = payload_ref[192:208, :].astype(F32)
    one = rows[0:1] + rows[1:2] + rows[2:3]
    two = rows[3:4] + rows[4:5] + rows[5:6]
    return one, two


def inside_body(xc_ref, k1_ref, q1_ref, kq2_ref, cum_ref, sp_ref, out_ref):
    length = xc_ref.shape[0]
    causal = lax.broadcasted_iota(jnp.int32, (BLOCK, BLOCK), 0) >= lax.broadcasted_iota(
        jnp.int32, (BLOCK, BLOCK), 1
    )
    first = lanes_of(1)
    contract = (((1,), (1,)), ((), ()))

    def step(b, none):
        at = pl.ds(pl.multiple_of(b * BLOCK, BLOCK), BLOCK)
        eight = pl.ds(pl.multiple_of(b * 8, 8), 8)
        rows, softs = cum_ref[eight, :], sp_ref[eight, :]
        columns = rows.T
        kq_two = kq2_ref[at, :].astype(F32)
        query_two = jnp.where(first, 0.0, kq_two).astype(BF16)
        key_two = pltpu.roll(kq_two, 64, 1).astype(BF16)
        scores = (
            lax.dot_general(q1_ref[at, :], k1_ref[at, :], contract, preferred_element_type=F32),
            lax.dot_general(query_two, key_two, contract, preferred_element_type=F32),
        )
        for group in range(2):
            values = xc_ref[at, group * 128 : group * 128 + 128]
            parts = []
            for inner in range(2):
                h = group * 2 + inner
                spans = jnp.where(causal, columns[:, h : h + 1] - rows[h : h + 1, :], -jnp.inf)
                weights = jnp.exp(spans) * (scores[group] * softs[h : h + 1, :])
                parts.append(jnp.dot(weights.astype(BF16), values, preferred_element_type=F32))
            out_ref[at, group * 128 : group * 128 + 128] = jnp.where(first, parts[0], parts[1])
        return none

    lax.fori_loop(0, length // BLOCK, step, 0)


def combine_body(y_ref, own_ref, b1_ref, b2_ref, b3_ref, pre_ref, lead_ref, total_ref):
    y = y_ref[3]
    refs = (own_ref, b1_ref, b2_ref, b3_ref)
    place = [lax.rem(y - k + 4, 4) for k in range(4)]
    logs = [logs_in(r) for r in refs]
    zero = jnp.zeros((1, 128), F32)

    def pick(flag, v):
        return jnp.where(flag, v, zero)

    leads = [zero, zero]
    pre_one = jnp.zeros((128, 128), F32)
    pre_two = jnp.zeros((64, 128), F32)
    tot_one = jnp.zeros((128, 128), F32)
    tot_two = jnp.zeros((64, 128), F32)
    for k in range(4):
        one = refs[k][0:128, :].astype(F32)
        two = refs[k][128:192, :].astype(F32)
        if k:
            flag = k <= y
            pre_one = pre_one + pick(flag, jnp.exp(leads[0])) * one
            pre_two = pre_two + pick(flag, jnp.exp(leads[1])) * two
            leads = [leads[g] + pick(flag, logs[k][g]) for g in range(2)]
        later = [zero, zero]
        for j in range(4):
            if j != k:
                flag = place[j] > place[k]
                later = [later[g] + pick(flag, logs[j][g]) for g in range(2)]
        tot_one = tot_one + jnp.exp(later[0]) * one
        tot_two = tot_two + jnp.exp(later[1]) * two
    pre_ref[0:128, :] = pre_one
    pre_ref[128:192, :] = pre_two
    lead_ref[0:1, :] = leads[0]
    lead_ref[1:2, :] = leads[1]
    tot_one = tot_one.astype(BF16)
    tot_two = tot_two.astype(BF16)
    tot_logs = log_rows(
        logs[0][0] + logs[1][0] + logs[2][0] + logs[3][0],
        logs[0][1] + logs[1][1] + logs[2][1] + logs[3][1],
    )
    for z in range(total_ref.shape[0]):
        total_ref[z, 0:128, :] = tot_one
        total_ref[z, 128:192, :] = tot_two
        total_ref[z, 192:208, :] = tot_logs


def mixed_body(
    pos_ref, in_ref, gate_ref, q1_ref, kq2_ref, cum_ref, s1_ref, s2_ref, lead_ref, gain_ref,
    pre_ref, ylead_ref, rows_ref, mine_ref, theirs_ref,
):
    c, z = pos_ref[1], pos_ref[2]
    far_one = jnp.zeros((128, 128), F32)
    far_two = jnp.zeros((64, 128), F32)
    run = [jnp.zeros((1, 128), F32)] * 2
    for k in reversed(range(rows_ref.shape[0] - 1)):
        flag = k < z
        r = rows_ref.at[k]
        scale = [jnp.where(flag, jnp.exp(v), 0.0) for v in run]
        far_one = far_one + scale[0] * r[0:128, :].astype(F32)
        far_two = far_two + scale[1] * r[128:192, :].astype(F32)
        logs = logs_in(r)
        run = [v + jnp.where(flag, more, 0.0) for v, more in zip(run, logs)]
    enter = (
        pre_ref[0:128, :] + jnp.exp(ylead_ref[0:1, :]) * far_one,
        jnp.concatenate(
            [
                jnp.zeros((64, 128), F32),
                pre_ref[128:192, :] + jnp.exp(ylead_ref[1:2, :]) * far_two,
            ],
            axis=0,
        ),
    )
    first = lanes_of(1)
    same_head = (
        (lax.broadcasted_iota(jnp.int32, (128, 128), 0) < 64)
        == (lax.broadcasted_iota(jnp.int32, (128, 128), 1) < 64)
    ).astype(BF16)
    blocks = in_ref.shape[0] // BLOCK
    half = blocks // 2

    def block(b, out_ref, to):
        at = pl.ds(pl.multiple_of(b * BLOCK, BLOCK), BLOCK)
        eight = pl.ds(pl.multiple_of(b * 8, 8), 8)
        columns = jnp.exp(cum_ref[eight, :].T)
        leads = jnp.exp(lead_ref[eight, :])
        for group in range(2):
            lane = slice(group * 128, group * 128 + 128)
            states = (s1_ref, s2_ref)[group][at, :].astype(F32)
            state = (states + leads[group : group + 1, :] * enter[group]).astype(BF16)
            query = (q1_ref, kq2_ref)[group][at, :]
            h = group * 2
            decay = jnp.where(first, columns[:, h : h + 1], columns[:, h + 1 : h + 2])
            mixer = in_ref[at, lane] + decay * jnp.dot(
                query, state, preferred_element_type=F32
            )
            gated = mixer * silu(gate_ref[at, lane].astype(F32))
            square = gated * gated
            hi = square.astype(BF16)
            low = (square - hi.astype(F32)).astype(BF16)
            mean = (
                jnp.dot(hi, same_head, preferred_element_type=F32)
                + jnp.dot(low, same_head, preferred_element_type=F32)
            ) * (1.0 / 64.0)
            scaled = gated * lax.rsqrt(mean + EPSILON) * gain_ref[group : group + 1, :]
            out_ref[to, lane] = scaled.astype(BF16)

    def step(i, none):
        to = pl.ds(pl.multiple_of(i * BLOCK, BLOCK), BLOCK)
        block(c * half + i, mine_ref, to)
        block((1 - c) * half + i, theirs_ref, to)
        return none

    lax.fori_loop(0, half, step, 0)


def projection_body(pos_ref, *refs):
    chunk_refs, (w_ref, res_ref, a_ref, b_ref, lhs) = refs[:8], refs[8:]
    x, c = pos_ref[0], pos_ref[1]
    for j, shift in enumerate((0, -1, 1, 2)):
        there = lax.rem(x + shift + 4, 4)
        for k in range(2):
            who = 2 * there + (c if k == 0 else 1 - c)
            lhs[:, pl.ds(pl.multiple_of(who * 256, 256), 256)] = chunk_refs[2 * j + k][...]
    total = res_ref[...].astype(F32) + jnp.dot(
        lhs[...], w_ref[...], preferred_element_type=F32
    )
    half = a_ref.shape[0]
    a_ref[...] = total[0:half].astype(BF16)
    b_ref[...] = total[half:].astype(BF16)


def normed_body(pos_ref, *refs):
    ins, gain_ref, out_ref = refs[:8], refs[8], refs[9]
    size = ins[0].shape[0]
    for k in range(2):
        full = [r[...].astype(F32) for r in ins[4 * k : 4 * k + 4]]
        square = sum(jnp.sum(v * v, axis=1, keepdims=True) for v in full)
        scale = lax.rsqrt(square * (1.0 / 2048.0) + EPSILON)
        for v, shift in zip(full, SHIFTS):
            at = lax.rem(pos_ref[0] + shift + 4, 4)
            lanes = pl.ds(pl.multiple_of(at * 512, 512), 512)
            out_ref[k * size : (k + 1) * size, lanes] = (v * scale * gain_ref[0:1, lanes]).astype(
                BF16
            )


def hidden_chunk(normed, wide_ref, hidden, lanes, width):
    depth = wide_ref.shape[1] * wide_ref.shape[2]
    gate, up = (
        jnp.dot(
            normed[...], wide_ref[part, :, :, lanes].reshape(depth, width),
            preferred_element_type=F32,
        )
        for part in range(2)
    )
    hidden[:, lanes] = (silu(gate) * up).astype(BF16)


def down_part(hidden, down, at, out_a, out_b):
    tall = down.shape[0] // 4
    rows = down[pl.ds(at * tall, tall), :, :].reshape(tall * down.shape[1], down.shape[2])
    contract = (((1,), (1,)), ((), ()))
    part = lax.dot_general(hidden[...], rows, contract, preferred_element_type=F32).astype(BF16)
    half = part.shape[0] // 2
    out_a[...] = part[0:half]
    out_b[...] = part[half:]


SHIFTS = (0, -1, 1, 2)
FAR_FIRST = (3, 1, 2, 0)


def hidden_body(
    pos_ref, normed, w_hbm, far_a, far_b, hidden, down, w_ref, sems
):
    width = w_hbm.shape[3] // 3
    whole = width // 256
    rest = width - whole * 256
    chunks = 2 * whole
    last = chunks * 256
    count = iter(range(sems.shape[0]))

    def copy(i, lo, hi, to, at):
        return pltpu.make_async_copy(
            w_hbm.at[:, i, :, lo:hi], to.at[:, :, at : at + hi - lo], sems.at[next(count)]
        )

    def pieces(n):
        for part in range(2):
            to, base = w_ref.at[part], part * width
            if n == chunks:
                for i in range(2):
                    yield copy(i, base + whole * 256, base + width, to, last + i * rest)
            else:
                lo = base + n % whole * 256
                yield copy(n // whole, lo, lo + 256, to, n * 256)

    def down_pieces():
        for i in range(2):
            base = 2 * width
            yield copy(i, base, base + whole * 256, down, i * whole * 256)
            yield copy(i, base + whole * 256, base + width, down, last + i * rest)

    def begin(copies):
        for each in copies:
            each.start()

    def finish(copies):
        for each in copies:
            each.wait()

    order = [list(pieces(n)) for n in range(chunks + 1)] + [list(down_pieces())]
    for each in order:
        begin(each)
    for n in range(chunks + 1):
        finish(order[n])
        wide = 256 if n < chunks else 2 * rest
        hidden_chunk(normed, w_ref, hidden, slice(n * 256, n * 256 + wide), wide)
    finish(order[chunks + 1])
    at = lax.rem(pos_ref[0] + SHIFTS[FAR_FIRST[0]] + 4, 4)
    down_part(hidden, down, at, far_a, far_b)


def near_body(pos_ref, hidden, down, *outs):
    for k, j in enumerate(FAR_FIRST[1:]):
        at = lax.rem(pos_ref[0] + SHIFTS[j] + 4, 4)
        down_part(hidden, down, at, outs[2 * k], outs[2 * k + 1])


def last_body(
    pos_ref, sa_ref, pa_ref, la_ref, ra_ref, sb_ref, pb_ref, lb_ref, rb_ref, mine_ref, theirs_ref
):
    c = pos_ref[1]
    size = sa_ref.shape[0]
    parts = ((sa_ref, pa_ref, la_ref, ra_ref), (sb_ref, pb_ref, lb_ref, rb_ref))
    for k, (s_ref, p_ref, left_ref, right_ref) in enumerate(parts):
        at = slice(k * size, (k + 1) * size)
        for ref, who in ((theirs_ref, 1 - c), (mine_ref, c)):
            lanes = pl.ds(pl.multiple_of(who * 256, 256), 256)
            total = (
                p_ref[:, lanes].astype(F32)
                + left_ref[:, lanes].astype(F32)
                + right_ref[:, lanes].astype(F32)
            )
            ref[at, :] = (s_ref[:, lanes].astype(F32) + 0.5 * total).astype(BF16)


def join_body(pos_ref, mine_ref, other_ref, out_ref, sems):
    c = pos_ref[1]
    size = mine_ref.shape[0]
    copies = []
    for k, (half, ref) in enumerate(((c, mine_ref), (1 - c, other_ref))):
        at = pl.ds(pl.multiple_of(half * size, size), size)
        copies.append(pltpu.make_async_copy(ref, out_ref.at[at, :], sems.at[k]))
    for each in copies:
        each.start()
    for each in copies:
        each.wait()


def turned(x, axis, distance):
    n = lax.axis_size(axis)
    return lax.ppermute(x, axis, [(i, (i + distance) % n) for i in range(n)])


def along_x(a, b):
    left_a, right_b = turned(a, "x", 1), turned(b, "x", -1)
    left_b, right_a = turned(b, "x", 1), turned(a, "x", -1)
    far_a, far_b = turned(left_a, "x", 1), turned(right_b, "x", -1)
    return (a, left_a, right_a, far_a), (b, left_b, right_b, far_b)


def shards(
    grouped_head_inputs,
    head_gate_inputs,
    unsmoothed_step,
    head_decay_rate,
    extra_log_decay,
    first_group_keys,
    first_group_queries,
    second_group_keys,
    second_group_queries,
    head_input_filter,
    first_group_filter,
    second_group_filter,
    head_norm_gain,
    output_weight,
    residual,
    channel_norm_gain,
    channel_gate_weight,
    channel_up_weight,
    channel_down_weight,
):
    length = grouped_head_inputs.shape[0]
    half = length // 2
    blocks = length // BLOCK
    xi = lax.axis_index("x").astype(jnp.int32)
    ci = lax.axis_index("c").astype(jnp.int32)
    yi = lax.axis_index("y").astype(jnp.int32)
    zi = lax.axis_index("z").astype(jnp.int32)
    pos = jnp.stack([xi, ci, zi, yi])

    def call(body, outs, args, name, scratch=(), spaces=None, limit=12, flops=None, loose=(), spilled=()):
        spaces = spaces or [pltpu.VMEM] * len(args)
        single = not isinstance(outs, tuple)
        outs = (outs,) if single else outs
        args = [
            a
            if s is pltpu.SMEM
            else pltpu.with_memory_space_constraint(a, pltpu.HBM if i in loose else s)
            for i, (a, s) in enumerate(zip(args, spaces))
        ]
        done = pl.pallas_call(
            body,
            out_shape=tuple(
                (pltpu.HBM if i in spilled else pltpu.VMEM)(o.shape, o.dtype)
                for i, o in enumerate(outs)
            ),
            in_specs=[pl.BlockSpec(memory_space=s) for s in spaces],
            out_specs=tuple(
                pl.BlockSpec(memory_space=pltpu.HBM if name == "join" else pltpu.VMEM)
                for _ in outs
            ),
            scratch_shapes=list(scratch),
            cost_estimate=flops
            and pl.CostEstimate(flops=flops, transcendentals=0, bytes_accessed=10**6),
            compiler_params=pltpu.CompilerParams(vmem_limit_bytes=limit * 2**20),
        )(*args)
        return done[0] if single else done

    def scalar_first(args):
        return [pltpu.SMEM] + [pltpu.VMEM] * (len(args) - 1)

    own_rows = jnp.concatenate(
        [channel_gate_weight, channel_up_weight, channel_down_weight], axis=1
    )
    all_w = lax.all_gather(own_rows, SP + ("c",), axis=0, tiled=True)
    x_flat = grouped_head_inputs.reshape(length, 256)
    k2t, q2t = second_group_keys.T, second_group_queries.T
    packed = pack_rim(x_flat, first_group_keys, first_group_queries, k2t, q2t)
    count = lax.axis_size(SP)
    rim = lax.ppermute(packed, SP, [(i, i + 1) for i in range(count - 1)])

    args = (
        head_decay_rate, x_flat, first_group_keys, first_group_queries, k2t, q2t, rim,
        head_input_filter, first_group_filter, second_group_filter,
        unsmoothed_step.transpose(1, 2, 0), extra_log_decay.transpose(1, 2, 0),
    )
    xc, k1c, q1c, kq2c, cum, soft, s1, s2, lead, end = call(
        states_body,
        (
            shape((length, 256), BF16),
            shape((length, 128), BF16),
            shape((length, 128), BF16),
            shape((length, 128), BF16),
            shape((8 * blocks, BLOCK), F32),
            shape((8 * blocks, BLOCK), F32),
            shape((length, 128), BF16),
            shape((length, 128), BF16),
            shape((8 * blocks, 128), F32),
            shape((208, 128), BF16),
        ),
        args,
        "states",
        loose=(1, 2, 3, 4, 5, 7, 8, 9, 10, 11),
        spilled=(1, 6, 7),
        scratch=(
            pltpu.VMEM((length + 8, 640), F32),
            pltpu.VMEM((8, 640), F32),
            pltpu.VMEM((8 * blocks, BLOCK), F32),
            pltpu.VMEM((8 * blocks, BLOCK), F32),
        ),
        spaces=scalar_first(args),
    )
    output_weight, residual, head_gate_inputs, end = lax.optimization_barrier(
        (output_weight, residual, head_gate_inputs, end)
    )
    before = [turned(end, "y", k) for k in (1, 2, 3)]
    args = (pos, end, *before)
    pre, ylead, total = call(
        combine_body,
        (shape((192, 128), F32), shape((8, 128), F32), shape((lax.axis_size("z"), 208, 128), BF16)),
        args,
        "combine",
        spaces=scalar_first(args),
    )
    rows = lax.all_to_all(total, "z", 0, 0, tiled=True)
    xc = lax.optimization_barrier((xc, total))[0]
    inside = call(
        inside_body,
        shape((length, 256), F32),
        (xc, k1c, q1c, kq2c, cum, soft),
        "inside",
        loose=(1,),
    )
    gates = head_gate_inputs.reshape(length, 256)
    args = (
        pos, inside, gates, q1c, kq2c, cum, s1, s2, lead, head_norm_gain, pre, ylead, rows
    )
    mine, theirs = call(
        mixed_body,
        (shape((half, 256), BF16), shape((half, 256), BF16)),
        args,
        "mixed",
        loose=(2, 6, 7, 9),
        spaces=scalar_first(args),
    )
    other = turned(theirs, "c", 1)

    w = output_weight.reshape(2, 8, 128, 256).transpose(1, 0, 2, 3).reshape(2048, 256)
    w_other = turned(w, "c", 1)
    res_other = turned(lax.dynamic_slice_in_dim(residual, (1 - ci) * half, half, axis=0), "c", 1)
    w_both = jnp.where(
        ci == 0, jnp.concatenate([w, w_other], 1), jnp.concatenate([w_other, w], 1)
    )
    res_mine = lax.dynamic_slice_in_dim(residual, ci * half, half, axis=0)
    res_both = jnp.where(
        ci == 0,
        jnp.concatenate([res_mine, res_other], 1),
        jnp.concatenate([res_other, res_mine], 1),
    )

    ours, others = along_x(mine, other)
    args = (pos, *(v for pair in zip(ours, others) for v in pair), w_both, res_both)
    stream_a, stream_b = call(
        projection_body,
        (shape((half // 2, 512), BF16), shape((half // 2, 512), BF16)),
        args,
        "projection",
        scratch=(pltpu.VMEM((half, 2048), BF16),),
        spaces=scalar_first(args),
    )
    all_a, all_b = along_x(stream_a, stream_b)
    quarter = shape((half // 2, 512), BF16)
    shard_rows, shard_cols = own_rows.shape
    all_w = all_w.reshape(-1, 2, shard_rows, shard_cols)
    wide = (all_w.shape[0], shard_rows, shard_cols // 3 * 2)

    normed = call(
        normed_body,
        shape((half, 2048), BF16),
        (pos, *all_a, *all_b, channel_norm_gain[None]),
        "normed",
        loose=(9,),
        spaces=[pltpu.SMEM] + [pltpu.VMEM] * 9,
    )
    pa3, pb3, hidden, down = call(
        hidden_body,
        (quarter, quarter, shape((half, wide[2]), BF16), shape(wide, BF16)),
        (pos, normed, all_w),
        "hidden",
        scratch=(
            pltpu.VMEM((2, *wide), BF16),
            pltpu.SemaphoreType.DMA((shard_cols // 3 // 256 * 4 + 8,)),
        ),
        spaces=[pltpu.SMEM, pltpu.VMEM, pltpu.HBM],
        limit=20,
    )
    far_a = turned(pa3, "x", 1)
    far_b = turned(pb3, "x", -1)
    pa1, pb1, pa2, pb2, pa0, pb0 = call(
        near_body,
        (quarter,) * 6,
        (pos, hidden, down),
        "near",
        spaces=[pltpu.SMEM] + [pltpu.VMEM] * 2,
    )
    left_b = turned(pb2, "x", 1)
    right_a = turned(pa1, "x", -1)
    sum_a = (pa2.astype(F32) + far_a.astype(F32)).astype(BF16)
    left_a = turned(sum_a, "x", 1)
    sum_b = (pb1.astype(F32) + far_b.astype(F32)).astype(BF16)
    right_b = turned(sum_b, "x", -1)
    mine, theirs = call(
        last_body,
        (shape((half, 256), BF16),) * 2,
        (pos, stream_a, pa0, left_a, right_a, stream_b, pb0, left_b, right_b),
        "last",
        spaces=[pltpu.SMEM] + [pltpu.VMEM] * 8,
    )
    other = turned(theirs, "c", 1)
    return call(
        join_body,
        shape((length, 256), BF16),
        (pos, mine, other),
        "join",
        spilled=(0,),
        scratch=(pltpu.SemaphoreType.DMA((2,)),),
        spaces=[pltpu.SMEM] + [pltpu.VMEM] * 2,
    )


def solution(mesh):
    sp, tp = mesh.devices.shape
    wide = Mesh(mesh.devices.reshape(sp // 4, 4, tp // 2, 2), ("z", "y", "x", "c"))

    return jax.shard_map(
        shards,
        mesh=wide,
        in_specs=(
            P(SP, None, TP),
            P(SP, None, TP),
            P(SP, None, TP),
            P(None, TP),
            P(SP, None, TP),
            P(SP, None),
            P(SP, None),
            P(SP, None),
            P(SP, None),
            P(None, None, TP),
            P(),
            P(),
            P(None, TP),
            P(None, None, TP),
            P(SP, TP),
            P(),
            P(SP, TP),
            P(SP, TP),
            P(SP, TP),
        ),
        out_specs=P(SP, TP),
        check_vma=False,
    )
```

```python
import functools

import jax
import jax.numpy as jnp
from jax import lax
from jax.experimental import pallas as pl
from jax.experimental.pallas import tpu as pltpu
from jax.sharding import Mesh, PartitionSpec as P


EPSILON = 1e-06
BLOCK = 128
F32 = jnp.float32
BF16 = jnp.bfloat16
SP = ("z", "y")
TP = ("x", "c")


def silu(v):
    return v * jax.nn.sigmoid(v)


def shape(dims, kind):
    return jax.ShapeDtypeStruct(dims, kind)


def pack_rim_body(x_ref, k1_ref, q1_ref, k2_ref, q2_ref, out_ref):
    out_ref[:, 0:256] = x_ref[...]
    out_ref[:, 256:384] = k1_ref[...]
    out_ref[:, 384:512] = q1_ref[...]
    both = jnp.concatenate([k2_ref[...], q2_ref[...]], axis=0).astype(F32)
    out_ref[:, 512:640] = both.T[112:128].astype(BF16)


def pack_rim(x_flat, k1, q1, k2t, q2t):
    rows = k1.shape[0] // 16 - 1
    cols = k2t.shape[1] // 128 - 1
    return pl.pallas_call(
        pack_rim_body,
        grid=(1,),
        in_specs=[
            pl.BlockSpec((16, 256), lambda i: (rows, 0)),
            pl.BlockSpec((16, 128), lambda i: (rows, 0)),
            pl.BlockSpec((16, 128), lambda i: (rows, 0)),
            pl.BlockSpec((64, 128), lambda i: (0, cols)),
            pl.BlockSpec((64, 128), lambda i: (0, cols)),
        ],
        out_specs=pl.BlockSpec((16, 640), lambda i: (0, 0)),
        out_shape=shape((16, 640), BF16),
        name="pack_rim",
    )(x_flat, k1, q1, k2t, q2t)


def lanes_of(rows):
    return lax.broadcasted_iota(jnp.int32, (rows, 128), 1) < 64


def three_parts(v):
    hi = v.astype(BF16)
    rest = v - hi.astype(F32)
    mid = rest.astype(BF16)
    low = (rest - mid.astype(F32)).astype(BF16)
    return hi.astype(F32), mid.astype(F32), low.astype(F32)


def states_body(
    rate_ref, x_ref, k1_ref, q1_ref, k2_ref, q2_ref, rim_ref, fx_ref, f1_ref, f2_ref, step_ref,
    extra_ref,
    xc_ref, k1c_ref, q1c_ref, kq2c_ref, cum_ref, sp_ref, s1_ref, s2_ref, lead_ref, end_ref,
    buf, filt, raw, more,
):
    length = x_ref.shape[0]
    blocks = length // BLOCK
    upper = (
        lax.broadcasted_iota(jnp.int32, (BLOCK, BLOCK), 0)
        <= lax.broadcasted_iota(jnp.int32, (BLOCK, BLOCK), 1)
    ).astype(F32)
    raw[...] = jnp.zeros(raw.shape, F32)
    more[...] = jnp.zeros(more.shape, F32)
    for b in range(blocks):
        for head in range(4):
            row = b * 8 + head
            at = slice(b * BLOCK, (b + 1) * BLOCK)
            raw[row : row + 1, :] = step_ref[head // 2, head % 2 : head % 2 + 1, at]
            more[row : row + 1, :] = extra_ref[head // 2, head % 2 : head % 2 + 1, at]
    place = lax.broadcasted_iota(jnp.int32, (8, BLOCK), 0)
    rate = jnp.zeros((8, BLOCK), F32)
    for head in range(4):
        rate = jnp.where(place == head, rate_ref[head // 2, head % 2], rate)
    values = raw[...]
    soft = jnp.maximum(values, 0.0) + jnp.log1p(jnp.exp(-jnp.abs(values)))
    sp_ref[...] = soft
    logs = more[...] - soft * jnp.concatenate([rate] * blocks, axis=0)
    cum_ref[...] = jnp.dot(
        logs, upper, precision=lax.Precision.HIGHEST, preferred_element_type=F32
    )
    for k in range(4):
        filt[k : k + 1, 0:128] = fx_ref[k, 0:1, :]
        filt[k : k + 1, 128:256] = fx_ref[k, 1:2, :]
        filt[k : k + 1, 256:384] = f1_ref[k, 0:1, :]
        filt[k : k + 1, 384:512] = f1_ref[k, 1:2, :]
        filt[k : k + 1, 512:640] = jnp.concatenate([f2_ref[k, 0:1, :], f2_ref[k, 1:2, :]], axis=1)
    buf[0:8, :] = rim_ref[8:16, :].astype(F32)
    first = lanes_of(1)

    def fill(b, none):
        at = pl.ds(pl.multiple_of(b * BLOCK, BLOCK), BLOCK)
        to = pl.ds(pl.multiple_of(b * BLOCK + 8, 8), BLOCK)
        buf[to, 0:256] = x_ref[at, :].astype(F32)
        buf[to, 256:384] = k1_ref[at, :].astype(F32)
        buf[to, 384:512] = q1_ref[at, :].astype(F32)
        both = jnp.concatenate([k2_ref[:, at], q2_ref[:, at]], axis=0).astype(F32)
        buf[to, 512:640] = both.T
        return none

    def step(b, carry):
        state_one, state_two, lead_one, lead_two = carry
        fill(b, 0)
        at = pl.ds(pl.multiple_of(b * BLOCK, BLOCK), BLOCK)
        around = pl.ds(pl.multiple_of(b * BLOCK, BLOCK), BLOCK + 8)

        def conv(lo, hi):
            window = buf[around, lo:hi]
            run = filt[0:1, lo:hi] * window[5 : 5 + BLOCK]
            for k in range(1, 4):
                run = run + filt[k : k + 1, lo:hi] * window[5 + k : 5 + k + BLOCK]
            return silu(run)

        x_one = conv(0, 128).astype(BF16)
        x_two = conv(128, 256).astype(BF16)
        xc_ref[at, 0:128] = x_one
        xc_ref[at, 128:256] = x_two
        k_one = conv(256, 384)
        k1c_ref[at, :] = k_one.astype(BF16)
        q1c_ref[at, :] = conv(384, 512).astype(BF16)
        kq_two = conv(512, 640)
        kq2c_ref[at, :] = kq_two.astype(BF16)
        s1_ref[at, :] = state_one.astype(BF16)
        s2_ref[at, :] = jnp.concatenate(
            [jnp.zeros((64, 128), BF16), state_two.astype(BF16)], axis=0
        )
        eight = pl.ds(pl.multiple_of(b * 8, 8), 8)
        lead_ref[eight, :] = jnp.concatenate(
            [lead_one, lead_two, jnp.zeros((6, 128), F32)], axis=0
        )
        rows, softs = cum_ref[eight, :], sp_ref[eight, :]
        tot = rows[:, 127:128]
        weight = jnp.exp(tot - rows) * softs
        key_one = k_one.T
        key_two = kq_two.T[0:64]
        ups = [
            jnp.dot(
                ((key_one if head < 2 else key_two) * weight[head : head + 1, :]).astype(BF16),
                x_one if head < 2 else x_two,
                preferred_element_type=F32,
            )
            for head in range(4)
        ]
        wide = jnp.broadcast_to(tot, (8, 128))
        tot_one = jnp.where(first, wide[0:1], wide[1:2])
        tot_two = jnp.where(first, wide[2:3], wide[3:4])
        return (
            state_one * jnp.exp(tot_one) + jnp.where(first, ups[0], ups[1]),
            state_two * jnp.exp(tot_two) + jnp.where(first, ups[2], ups[3]),
            lead_one + tot_one,
            lead_two + tot_two,
        )

    state_one, state_two, lead_one, lead_two = lax.fori_loop(
        0,
        blocks,
        step,
        (
            jnp.zeros((128, 128), F32),
            jnp.zeros((64, 128), F32),
            jnp.zeros((1, 128), F32),
            jnp.zeros((1, 128), F32),
        ),
    )
    end_ref[0:128, :] = state_one.astype(BF16)
    end_ref[128:192, :] = state_two.astype(BF16)
    end_ref[192:208, :] = log_rows(lead_one, lead_two)


def log_rows(one, two):
    parts = three_parts(one) + three_parts(two)
    return jnp.concatenate(list(parts) + [jnp.zeros((10, 128), F32)], axis=0).astype(BF16)


def logs_in(payload_ref):
    rows = payload_ref[192:208, :].astype(F32)
    one = rows[0:1] + rows[1:2] + rows[2:3]
    two = rows[3:4] + rows[4:5] + rows[5:6]
    return one, two


def inside_body(xc_ref, k1_ref, q1_ref, kq2_ref, cum_ref, sp_ref, out_ref):
    length = xc_ref.shape[0]
    causal = lax.broadcasted_iota(jnp.int32, (BLOCK, BLOCK), 0) >= lax.broadcasted_iota(
        jnp.int32, (BLOCK, BLOCK), 1
    )
    first = lanes_of(1)
    contract = (((1,), (1,)), ((), ()))

    def step(b, none):
        at = pl.ds(pl.multiple_of(b * BLOCK, BLOCK), BLOCK)
        eight = pl.ds(pl.multiple_of(b * 8, 8), 8)
        rows, softs = cum_ref[eight, :], sp_ref[eight, :]
        columns = rows.T
        kq_two = kq2_ref[at, :].astype(F32)
        query_two = jnp.where(first, 0.0, kq_two).astype(BF16)
        key_two = pltpu.roll(kq_two, 64, 1).astype(BF16)
        scores = (
            lax.dot_general(q1_ref[at, :], k1_ref[at, :], contract, preferred_element_type=F32),
            lax.dot_general(query_two, key_two, contract, preferred_element_type=F32),
        )
        for group in range(2):
            values = xc_ref[at, group * 128 : group * 128 + 128]
            parts = []
            for inner in range(2):
                h = group * 2 + inner
                spans = jnp.where(causal, columns[:, h : h + 1] - rows[h : h + 1, :], -jnp.inf)
                weights = jnp.exp(spans) * (scores[group] * softs[h : h + 1, :])
                parts.append(jnp.dot(weights.astype(BF16), values, preferred_element_type=F32))
            out_ref[at, group * 128 : group * 128 + 128] = jnp.where(first, parts[0], parts[1])
        return none

    lax.fori_loop(0, length // BLOCK, step, 0)


def combine_body(y_ref, own_ref, b1_ref, b2_ref, b3_ref, pre_ref, lead_ref, total_ref):
    y = y_ref[3]
    refs = (own_ref, b1_ref, b2_ref, b3_ref)
    place = [lax.rem(y - k + 4, 4) for k in range(4)]
    logs = [logs_in(r) for r in refs]
    zero = jnp.zeros((1, 128), F32)

    def pick(flag, v):
        return jnp.where(flag, v, zero)

    leads = [zero, zero]
    pre_one = jnp.zeros((128, 128), F32)
    pre_two = jnp.zeros((64, 128), F32)
    tot_one = jnp.zeros((128, 128), F32)
    tot_two = jnp.zeros((64, 128), F32)
    for k in range(4):
        one = refs[k][0:128, :].astype(F32)
        two = refs[k][128:192, :].astype(F32)
        if k:
            flag = k <= y
            pre_one = pre_one + pick(flag, jnp.exp(leads[0])) * one
            pre_two = pre_two + pick(flag, jnp.exp(leads[1])) * two
            leads = [leads[g] + pick(flag, logs[k][g]) for g in range(2)]
        later = [zero, zero]
        for j in range(4):
            if j != k:
                flag = place[j] > place[k]
                later = [later[g] + pick(flag, logs[j][g]) for g in range(2)]
        tot_one = tot_one + jnp.exp(later[0]) * one
        tot_two = tot_two + jnp.exp(later[1]) * two
    pre_ref[0:128, :] = pre_one
    pre_ref[128:192, :] = pre_two
    lead_ref[0:1, :] = leads[0]
    lead_ref[1:2, :] = leads[1]
    tot_one = tot_one.astype(BF16)
    tot_two = tot_two.astype(BF16)
    tot_logs = log_rows(
        logs[0][0] + logs[1][0] + logs[2][0] + logs[3][0],
        logs[0][1] + logs[1][1] + logs[2][1] + logs[3][1],
    )
    for z in range(total_ref.shape[0]):
        total_ref[z, 0:128, :] = tot_one
        total_ref[z, 128:192, :] = tot_two
        total_ref[z, 192:208, :] = tot_logs


def mixed_body(
    pos_ref, in_ref, gate_ref, q1_ref, kq2_ref, cum_ref, s1_ref, s2_ref, lead_ref, gain_ref,
    pre_ref, ylead_ref, rows_ref, mine_ref, theirs_ref,
):
    c, z = pos_ref[1], pos_ref[2]
    far_one = jnp.zeros((128, 128), F32)
    far_two = jnp.zeros((64, 128), F32)
    run = [jnp.zeros((1, 128), F32)] * 2
    for k in reversed(range(rows_ref.shape[0] - 1)):
        flag = k < z
        r = rows_ref.at[k]
        scale = [jnp.where(flag, jnp.exp(v), 0.0) for v in run]
        far_one = far_one + scale[0] * r[0:128, :].astype(F32)
        far_two = far_two + scale[1] * r[128:192, :].astype(F32)
        logs = logs_in(r)
        run = [v + jnp.where(flag, more, 0.0) for v, more in zip(run, logs)]
    enter = (
        pre_ref[0:128, :] + jnp.exp(ylead_ref[0:1, :]) * far_one,
        jnp.concatenate(
            [
                jnp.zeros((64, 128), F32),
                pre_ref[128:192, :] + jnp.exp(ylead_ref[1:2, :]) * far_two,
            ],
            axis=0,
        ),
    )
    first = lanes_of(1)
    same_head = (
        (lax.broadcasted_iota(jnp.int32, (128, 128), 0) < 64)
        == (lax.broadcasted_iota(jnp.int32, (128, 128), 1) < 64)
    ).astype(BF16)
    blocks = in_ref.shape[0] // BLOCK
    half = blocks // 2

    def block(b, out_ref, to):
        at = pl.ds(pl.multiple_of(b * BLOCK, BLOCK), BLOCK)
        eight = pl.ds(pl.multiple_of(b * 8, 8), 8)
        columns = jnp.exp(cum_ref[eight, :].T)
        leads = jnp.exp(lead_ref[eight, :])
        for group in range(2):
            lane = slice(group * 128, group * 128 + 128)
            states = (s1_ref, s2_ref)[group][at, :].astype(F32)
            state = (states + leads[group : group + 1, :] * enter[group]).astype(BF16)
            query = (q1_ref, kq2_ref)[group][at, :]
            h = group * 2
            decay = jnp.where(first, columns[:, h : h + 1], columns[:, h + 1 : h + 2])
            mixer = in_ref[at, lane] + decay * jnp.dot(
                query, state, preferred_element_type=F32
            )
            gated = mixer * silu(gate_ref[at, lane].astype(F32))
            square = gated * gated
            hi = square.astype(BF16)
            low = (square - hi.astype(F32)).astype(BF16)
            mean = (
                jnp.dot(hi, same_head, preferred_element_type=F32)
                + jnp.dot(low, same_head, preferred_element_type=F32)
            ) * (1.0 / 64.0)
            scaled = gated * lax.rsqrt(mean + EPSILON) * gain_ref[group : group + 1, :]
            out_ref[to, lane] = scaled.astype(BF16)

    def step(i, none):
        to = pl.ds(pl.multiple_of(i * BLOCK, BLOCK), BLOCK)
        block(c * half + i, mine_ref, to)
        block((1 - c) * half + i, theirs_ref, to)
        return none

    lax.fori_loop(0, half, step, 0)


def projection_body(pos_ref, *refs):
    chunk_refs, (w_ref, res_ref, a_ref, b_ref, lhs) = refs[:8], refs[8:]
    x, c = pos_ref[0], pos_ref[1]
    for j, shift in enumerate((0, -1, 1, 2)):
        there = lax.rem(x + shift + 4, 4)
        for k in range(2):
            who = 2 * there + (c if k == 0 else 1 - c)
            lhs[:, pl.ds(pl.multiple_of(who * 256, 256), 256)] = chunk_refs[2 * j + k][...]
    total = res_ref[...].astype(F32) + jnp.dot(
        lhs[...], w_ref[...], preferred_element_type=F32
    )
    half = a_ref.shape[0]
    a_ref[...] = total[0:half].astype(BF16)
    b_ref[...] = total[half:].astype(BF16)


def normed_body(pos_ref, *refs):
    ins, gain_ref, out_ref = refs[:8], refs[8], refs[9]
    size = ins[0].shape[0]
    for k in range(2):
        full = [r[...].astype(F32) for r in ins[4 * k : 4 * k + 4]]
        square = sum(jnp.sum(v * v, axis=1, keepdims=True) for v in full)
        scale = lax.rsqrt(square * (1.0 / 2048.0) + EPSILON)
        for v, shift in zip(full, SHIFTS):
            at = lax.rem(pos_ref[0] + shift + 4, 4)
            lanes = pl.ds(pl.multiple_of(at * 512, 512), 512)
            out_ref[k * size : (k + 1) * size, lanes] = (v * scale * gain_ref[0:1, lanes]).astype(
                BF16
            )


def hidden_chunk(normed, wide_ref, hidden, lanes, width):
    depth = wide_ref.shape[1] * wide_ref.shape[2]
    gate, up = (
        jnp.dot(
            normed[...], wide_ref[part, :, :, lanes].reshape(depth, width),
            preferred_element_type=F32,
        )
        for part in range(2)
    )
    hidden[:, lanes] = (silu(gate) * up).astype(BF16)


def down_part(hidden, down, at, out_a, out_b):
    tall = down.shape[0] // 4
    rows = down[pl.ds(at * tall, tall), :, :].reshape(tall * down.shape[1], down.shape[2])
    contract = (((1,), (1,)), ((), ()))
    part = lax.dot_general(hidden[...], rows, contract, preferred_element_type=F32).astype(BF16)
    half = part.shape[0] // 2
    out_a[...] = part[0:half]
    out_b[...] = part[half:]


SHIFTS = (0, -1, 1, 2)
FAR_FIRST = (3, 1, 2, 0)


def hidden_body(
    pos_ref, normed, w_hbm, far_a, far_b, hidden, down, w_ref, sems
):
    width = w_hbm.shape[3] // 3
    whole = width // 256
    rest = width - whole * 256
    chunks = 2 * whole
    last = chunks * 256
    count = iter(range(sems.shape[0]))

    def copy(i, lo, hi, to, at):
        return pltpu.make_async_copy(
            w_hbm.at[:, i, :, lo:hi], to.at[:, :, at : at + hi - lo], sems.at[next(count)]
        )

    def pieces(n):
        for part in range(2):
            to, base = w_ref.at[part], part * width
            if n == chunks:
                for i in range(2):
                    yield copy(i, base + whole * 256, base + width, to, last + i * rest)
            else:
                lo = base + n % whole * 256
                yield copy(n // whole, lo, lo + 256, to, n * 256)

    def down_pieces():
        for i in range(2):
            base = 2 * width
            yield copy(i, base, base + whole * 256, down, i * whole * 256)
            yield copy(i, base + whole * 256, base + width, down, last + i * rest)

    def begin(copies):
        for each in copies:
            each.start()

    def finish(copies):
        for each in copies:
            each.wait()

    order = [list(pieces(n)) for n in range(chunks + 1)] + [list(down_pieces())]
    for each in order:
        begin(each)
    for n in range(chunks + 1):
        finish(order[n])
        wide = 256 if n < chunks else 2 * rest
        hidden_chunk(normed, w_ref, hidden, slice(n * 256, n * 256 + wide), wide)
    finish(order[chunks + 1])
    at = lax.rem(pos_ref[0] + SHIFTS[FAR_FIRST[0]] + 4, 4)
    down_part(hidden, down, at, far_a, far_b)


def near_body(pos_ref, hidden, down, *outs):
    for k, j in enumerate(FAR_FIRST[1:]):
        at = lax.rem(pos_ref[0] + SHIFTS[j] + 4, 4)
        down_part(hidden, down, at, outs[2 * k], outs[2 * k + 1])


def last_body(
    other, pos_ref, sa_ref, pa_ref, la_ref, ra_ref, sb_ref, pb_ref, lb_ref, rb_ref, out_ref
):
    c = pos_ref[1]
    size = sa_ref.shape[0]
    lanes = pl.ds(pl.multiple_of((1 - c if other else c) * 256, 256), 256)
    parts = ((sa_ref, pa_ref, la_ref, ra_ref), (sb_ref, pb_ref, lb_ref, rb_ref))
    for k, (s_ref, p_ref, left_ref, right_ref) in enumerate(parts):
        total = (
            p_ref[:, lanes].astype(F32)
            + left_ref[:, lanes].astype(F32)
            + right_ref[:, lanes].astype(F32)
        )
        out_ref[k * size : (k + 1) * size, :] = (
            s_ref[:, lanes].astype(F32) + 0.5 * total
        ).astype(BF16)


def join_body(pos_ref, mine_ref, other_ref, out_ref, sems):
    c = pos_ref[1]
    size = mine_ref.shape[0]
    copies = []
    for k, (half, ref) in enumerate(((c, mine_ref), (1 - c, other_ref))):
        at = pl.ds(pl.multiple_of(half * size, size), size)
        copies.append(pltpu.make_async_copy(ref, out_ref.at[at, :], sems.at[k]))
    for each in copies:
        each.start()
    for each in copies:
        each.wait()


def turned(x, axis, distance):
    n = lax.axis_size(axis)
    return lax.ppermute(x, axis, [(i, (i + distance) % n) for i in range(n)])


def along_x(a, b):
    left_a, right_b = turned(a, "x", 1), turned(b, "x", -1)
    left_b, right_a = turned(b, "x", 1), turned(a, "x", -1)
    far_a, far_b = turned(left_a, "x", 1), turned(right_b, "x", -1)
    return (a, left_a, right_a, far_a), (b, left_b, right_b, far_b)


def shards(
    grouped_head_inputs,
    head_gate_inputs,
    unsmoothed_step,
    head_decay_rate,
    extra_log_decay,
    first_group_keys,
    first_group_queries,
    second_group_keys,
    second_group_queries,
    head_input_filter,
    first_group_filter,
    second_group_filter,
    head_norm_gain,
    output_weight,
    residual,
    channel_norm_gain,
    channel_gate_weight,
    channel_up_weight,
    channel_down_weight,
):
    length = grouped_head_inputs.shape[0]
    half = length // 2
    blocks = length // BLOCK
    xi = lax.axis_index("x").astype(jnp.int32)
    ci = lax.axis_index("c").astype(jnp.int32)
    yi = lax.axis_index("y").astype(jnp.int32)
    zi = lax.axis_index("z").astype(jnp.int32)
    pos = jnp.stack([xi, ci, zi, yi])

    def call(body, outs, args, name, scratch=(), spaces=None, limit=12, flops=None, loose=(), spilled=()):
        spaces = spaces or [pltpu.VMEM] * len(args)
        single = not isinstance(outs, tuple)
        outs = (outs,) if single else outs
        args = [
            a
            if s is pltpu.SMEM
            else pltpu.with_memory_space_constraint(a, pltpu.HBM if i in loose else s)
            for i, (a, s) in enumerate(zip(args, spaces))
        ]
        done = pl.pallas_call(
            body,
            out_shape=tuple(
                (pltpu.HBM if i in spilled else pltpu.VMEM)(o.shape, o.dtype)
                for i, o in enumerate(outs)
            ),
            in_specs=[pl.BlockSpec(memory_space=s) for s in spaces],
            out_specs=tuple(
                pl.BlockSpec(memory_space=pltpu.HBM if name == "join" else pltpu.VMEM)
                for _ in outs
            ),
            scratch_shapes=list(scratch),
            cost_estimate=flops
            and pl.CostEstimate(flops=flops, transcendentals=0, bytes_accessed=10**6),
            compiler_params=pltpu.CompilerParams(vmem_limit_bytes=limit * 2**20),
        )(*args)
        return done[0] if single else done

    def scalar_first(args):
        return [pltpu.SMEM] + [pltpu.VMEM] * (len(args) - 1)

    own_rows = jnp.concatenate(
        [channel_gate_weight, channel_up_weight, channel_down_weight], axis=1
    )
    all_w = lax.all_gather(own_rows, SP + ("c",), axis=0, tiled=True)
    x_flat = grouped_head_inputs.reshape(length, 256)
    k2t, q2t = second_group_keys.T, second_group_queries.T
    packed = pack_rim(x_flat, first_group_keys, first_group_queries, k2t, q2t)
    count = lax.axis_size(SP)
    rim = lax.ppermute(packed, SP, [(i, i + 1) for i in range(count - 1)])

    args = (
        head_decay_rate, x_flat, first_group_keys, first_group_queries, k2t, q2t, rim,
        head_input_filter, first_group_filter, second_group_filter,
        unsmoothed_step.transpose(1, 2, 0), extra_log_decay.transpose(1, 2, 0),
    )
    xc, k1c, q1c, kq2c, cum, soft, s1, s2, lead, end = call(
        states_body,
        (
            shape((length, 256), BF16),
            shape((length, 128), BF16),
            shape((length, 128), BF16),
            shape((length, 128), BF16),
            shape((8 * blocks, BLOCK), F32),
            shape((8 * blocks, BLOCK), F32),
            shape((length, 128), BF16),
            shape((length, 128), BF16),
            shape((8 * blocks, 128), F32),
            shape((208, 128), BF16),
        ),
        args,
        "states",
        loose=(1, 2, 3, 4, 5, 7, 8, 9, 10, 11),
        spilled=(1, 6, 7),
        scratch=(
            pltpu.VMEM((length + 8, 640), F32),
            pltpu.VMEM((8, 640), F32),
            pltpu.VMEM((8 * blocks, BLOCK), F32),
            pltpu.VMEM((8 * blocks, BLOCK), F32),
        ),
        spaces=scalar_first(args),
    )
    output_weight, residual, head_gate_inputs, end = lax.optimization_barrier(
        (output_weight, residual, head_gate_inputs, end)
    )
    before = [turned(end, "y", k) for k in (1, 2, 3)]
    args = (pos, end, *before)
    pre, ylead, total = call(
        combine_body,
        (shape((192, 128), F32), shape((8, 128), F32), shape((lax.axis_size("z"), 208, 128), BF16)),
        args,
        "combine",
        spaces=scalar_first(args),
    )
    rows = lax.all_to_all(total, "z", 0, 0, tiled=True)
    xc = lax.optimization_barrier((xc, total))[0]
    inside = call(
        inside_body,
        shape((length, 256), F32),
        (xc, k1c, q1c, kq2c, cum, soft),
        "inside",
        loose=(1,),
    )
    gates = head_gate_inputs.reshape(length, 256)
    args = (
        pos, inside, gates, q1c, kq2c, cum, s1, s2, lead, head_norm_gain, pre, ylead, rows
    )
    mine, theirs = call(
        mixed_body,
        (shape((half, 256), BF16), shape((half, 256), BF16)),
        args,
        "mixed",
        loose=(2, 6, 7, 9),
        spaces=scalar_first(args),
    )
    other = turned(theirs, "c", 1)

    w = output_weight.reshape(2, 8, 128, 256).transpose(1, 0, 2, 3).reshape(2048, 256)
    w_other = turned(w, "c", 1)
    res_other = turned(lax.dynamic_slice_in_dim(residual, (1 - ci) * half, half, axis=0), "c", 1)
    w_both = jnp.where(
        ci == 0, jnp.concatenate([w, w_other], 1), jnp.concatenate([w_other, w], 1)
    )
    res_mine = lax.dynamic_slice_in_dim(residual, ci * half, half, axis=0)
    res_both = jnp.where(
        ci == 0,
        jnp.concatenate([res_mine, res_other], 1),
        jnp.concatenate([res_other, res_mine], 1),
    )

    ours, others = along_x(mine, other)
    args = (pos, *(v for pair in zip(ours, others) for v in pair), w_both, res_both)
    stream_a, stream_b = call(
        projection_body,
        (shape((half // 2, 512), BF16), shape((half // 2, 512), BF16)),
        args,
        "projection",
        scratch=(pltpu.VMEM((half, 2048), BF16),),
        spaces=scalar_first(args),
    )
    all_a, all_b = along_x(stream_a, stream_b)
    quarter = shape((half // 2, 512), BF16)
    shard_rows, shard_cols = own_rows.shape
    all_w = all_w.reshape(-1, 2, shard_rows, shard_cols)
    wide = (all_w.shape[0], shard_rows, shard_cols // 3 * 2)

    normed = call(
        normed_body,
        shape((half, 2048), BF16),
        (pos, *all_a, *all_b, channel_norm_gain[None]),
        "normed",
        loose=(9,),
        spaces=[pltpu.SMEM] + [pltpu.VMEM] * 9,
    )
    pa3, pb3, hidden, down = call(
        hidden_body,
        (quarter, quarter, shape((half, wide[2]), BF16), shape(wide, BF16)),
        (pos, normed, all_w),
        "hidden",
        scratch=(
            pltpu.VMEM((2, *wide), BF16),
            pltpu.SemaphoreType.DMA((shard_cols // 3 // 256 * 4 + 8,)),
        ),
        spaces=[pltpu.SMEM, pltpu.VMEM, pltpu.HBM],
        limit=20,
    )
    far_a = turned(pa3, "x", 1)
    far_b = turned(pb3, "x", -1)
    pa1, pb1, pa2, pb2, pa0, pb0 = call(
        near_body,
        (quarter,) * 6,
        (pos, hidden, down),
        "near",
        spaces=[pltpu.SMEM] + [pltpu.VMEM] * 2,
    )
    left_b = turned(pb2, "x", 1)
    right_a = turned(pa1, "x", -1)
    sum_a = (pa2.astype(F32) + far_a.astype(F32)).astype(BF16)
    left_a = turned(sum_a, "x", 1)
    sum_b = (pb1.astype(F32) + far_b.astype(F32)).astype(BF16)
    right_b = turned(sum_b, "x", -1)

    def last(other, name):
        return call(
            functools.partial(last_body, other),
            shape((half, 256), BF16),
            (pos, stream_a, pa0, left_a, right_a, stream_b, pb0, left_b, right_b),
            name,
            spaces=[pltpu.SMEM] + [pltpu.VMEM] * 8,
        )

    theirs = last(True, "theirs")
    other = turned(theirs, "c", 1)
    mine = last(False, "mine")
    return call(
        join_body,
        shape((length, 256), BF16),
        (pos, mine, other),
        "join",
        spilled=(0,),
        scratch=(pltpu.SemaphoreType.DMA((2,)),),
        spaces=[pltpu.SMEM] + [pltpu.VMEM] * 2,
    )


def solution(mesh):
    sp, tp = mesh.devices.shape
    wide = Mesh(mesh.devices.reshape(sp // 4, 4, tp // 2, 2), ("z", "y", "x", "c"))

    return jax.shard_map(
        shards,
        mesh=wide,
        in_specs=(
            P(SP, None, TP),
            P(SP, None, TP),
            P(SP, None, TP),
            P(None, TP),
            P(SP, None, TP),
            P(SP, None),
            P(SP, None),
            P(SP, None),
            P(SP, None),
            P(None, None, TP),
            P(),
            P(),
            P(None, TP),
            P(None, None, TP),
            P(SP, TP),
            P(),
            P(SP, TP),
            P(SP, TP),
            P(SP, TP),
        ),
        out_specs=P(SP, TP),
        check_vma=False,
    )
```
